128 devices in a mesh: ep: 16 (over z, x), tp: 8 (over y, core).
Axes of the slice: x: 4, y: 4, z: 4, core: 2. Of those that a mesh axis runs over, the one named last changes fastest.
Arguments:
- mix_query: bfloat16 [32768, 2048], P('ep', 'tp'), may hold values from -6 to 6
- mix_key: bfloat16 [32768, 2048], P('ep', 'tp'), may hold values from -6 to 6
- mix_value: bfloat16 [32768, 2048], P('ep', 'tp'), may hold values from -6 to 6
- mix_gate: bfloat16 [32768, 2048], P('ep', 'tp'), may hold values from -6 to 6
- log_decay: float32 [32768, 8], P('ep', 'tp'), may hold values from -1 to 0, as said below
- ret_gain: float32 [2048], P('tp'), may hold values from 0.1 to 1.9
- w_out: bfloat16 [2048, 2048], replicated, may hold values from -0.125 to 0.125
- moe_in: bfloat16 [4096, 2048], P(('ep', 'tp')), may hold values from -6 to 6
- route_ids: int32 [4096, 2], P(('ep', 'tp')), may hold values from 0 to 15, as said below
- route_weights: float32 [4096, 2], P(('ep', 'tp')), may hold values from 0.1 to 1
- moe_gain: float32 [2048], replicated, may hold values from 0.1 to 1.9
- w_gate: bfloat16 [16, 2048, 7168], P('ep', None, 'tp'), may hold values from -0.125 to 0.125
- w_up: bfloat16 [16, 2048, 7168], P('ep', None, 'tp'), may hold values from -0.125 to 0.125
- w_down: bfloat16 [16, 7168, 2048], P('ep', 'tp'), may hold values from -0.0625 to 0.0625
Outputs:
- mix_out: bfloat16 [32768, 2048], P(('ep', 'tp'))
- moe_out: bfloat16 [4096, 2048], P(('ep', 'tp'))
The draws below stay inside these ranges and needn't reach their ends.
Inputs may be any that keep to these rules, and one draw needn't show every extreme that they name: `log_decay`: log of a decay. `route_ids`: each row names 2 different experts. Among the rows of one device no expert is named by more than 8 rows, and one expert is named by exactly 8 rows of every device.
All inputs are finite; a program needn't handle non-finite values.
Results may differ from the reference program's by a relative error of at most 0.015.
Values may be sent and summed in bfloat16 or wider, within the bound.
No kernel may reach another device: no remote copies, remote signals or barrier semaphores. Data moves between devices by JAX's collectives and lax.ppermute only.
A program may use at most 128 MiB of HBM per device.

```python
import math
import jax
import jax.numpy as jnp
from jax import lax

D = 2048
FF = 7168
RETENTION_HEADS = 8
HEAD_DIM = 256
BLOCK = 512
TOP = 2
SEQ_DEV = 2048
MOE_DEV = 32
SEQUENCE_LENGTH = 32768
MOE_TOK = 4096
EXPERTS = 16
CAP = 8
N_TP = 8


def block_permutation(perm_key, length):
    return jax.random.permutation(perm_key, length)


def draw_route_ids(key, part):
    block_count = MOE_TOK // MOE_DEV
    half_cap = CAP // 2
    pair_count = (EXPERTS - 2) // 2
    base_key = jax.random.fold_in(key, 31)
    key_star, key_order, key_delta, key_shuffle = jax.random.split(base_key, 4)
    star = jax.random.randint(key_star, (), 0, EXPERTS)
    others = (star + 1 + jnp.arange(EXPERTS - 1, dtype=jnp.int32)) % EXPERTS
    order_keys = jax.random.split(key_order, block_count)
    orders = jax.vmap(block_permutation, in_axes=(0, None))(order_keys, EXPERTS - 1)
    ranked = others[orders]
    delta = jax.random.randint(key_delta, (block_count, pair_count), 0, half_cap + 1)
    pair_counts = jnp.stack([half_cap + delta, half_cap - delta], axis=-1).reshape(block_count, 2 * pair_count)
    counts = jnp.concatenate([jnp.full((block_count, 1), CAP, jnp.int32), pair_counts.astype(jnp.int32), jnp.zeros((block_count, 1), jnp.int32)], axis=1)
    listed = jnp.concatenate([jnp.full((block_count, 1), star, jnp.int32), ranked.astype(jnp.int32)], axis=1)
    bounds = jnp.cumsum(counts, axis=1)
    slots = jnp.arange(2 * MOE_DEV, dtype=jnp.int32)
    position = jnp.sum((slots[None, :, None] >= bounds[:, None, :]).astype(jnp.int32), axis=-1)
    chosen = jnp.take_along_axis(listed, position, axis=1)
    paired = jnp.stack([chosen[:, :MOE_DEV], chosen[:, MOE_DEV:]], axis=-1)
    shuffle_keys = jax.random.split(key_shuffle, block_count)
    shuffles = jax.vmap(block_permutation, in_axes=(0, None))(shuffle_keys, MOE_DEV)
    paired = jnp.take_along_axis(paired, shuffles[:, :, None], axis=1)
    return paired.reshape(MOE_TOK, TOP).astype(jnp.int32)


def draw_log_decay(key, part):
    base_key = jax.random.fold_in(key, 53)
    random_keys = jax.random.split(base_key, 6)
    fast_heads = jax.random.uniform(random_keys[0], (RETENTION_HEADS,)) < 0.5
    fast_rate = 1.0 / jax.random.uniform(random_keys[1], (RETENTION_HEADS,), minval=30.0, maxval=100.0)
    slow_rate = jax.random.uniform(random_keys[2], (RETENTION_HEADS,), minval=0.05, maxval=0.2) * math.log(10.0) / SEQUENCE_LENGTH
    per_head_decay = jnp.where(fast_heads, fast_rate, slow_rate)
    device_factor = jnp.exp(jax.random.uniform(random_keys[3], (SEQUENCE_LENGTH // SEQ_DEV,), minval=math.log(0.5), maxval=math.log(2.0)))
    position_index = jnp.arange(SEQUENCE_LENGTH, dtype=jnp.int32)
    decay_factor_lookup = device_factor[position_index // SEQ_DEV]
    spike_position = jax.random.randint(random_keys[4], (RETENTION_HEADS, 2), 0, SEQUENCE_LENGTH)
    spike_length = jnp.log(jax.random.uniform(random_keys[5], (RETENTION_HEADS, 2), minval=0.5, maxval=0.8))
    spike_matches = position_index[:, None, None] == spike_position[None, :, :]
    spike_list = jnp.sum(jnp.where(spike_matches, spike_length[None, :, :], 0.0), axis=-1)
    return (-per_head_decay[None, :] * decay_factor_lookup[:, None] + spike_list).astype(jnp.float32)


def steps_of(rng, dims, shards, smallest, high):
    def one(axis_at, shards_of):
        draws = jax.random.uniform(jax.random.fold_in(jax.random.fold_in(rng, 6), axis_at), (shards_of,), jnp.float32, smallest / len(shards), high / len(shards))
        return jnp.repeat(jnp.exp(draws), dims[axis_at] // shards_of).reshape((-1,) + (1,) * (len(dims) - axis_at - 1))

    gain = one(*shards[0])
    for cut in shards[1:]:
        gain = gain * one(*cut)
    return gain


def noise(rng, dims, width, most, cuts=(), kind=jnp.bfloat16):
    drawn = width * jax.random.normal(rng, dims, jnp.float32)
    if cuts:
        drawn = drawn * steps_of(rng, dims, cuts, -0.22, 0.18)
    return jnp.clip(drawn, -most, most).astype(kind)


def setup_inputs(seed: int = 0) -> dict:
    splits = jax.random.split(jax.random.key(seed), 15)
    mix_query = noise(splits[0], (SEQUENCE_LENGTH, RETENTION_HEADS * HEAD_DIM), 1.0, 6.0, ((0, 16), (1, 8)))
    mix_key = noise(splits[1], (SEQUENCE_LENGTH, RETENTION_HEADS * HEAD_DIM), 1.0, 6.0, ((0, 16), (1, 8)))
    mix_value = noise(splits[2], (SEQUENCE_LENGTH, RETENTION_HEADS * HEAD_DIM), 1.0, 6.0, ((0, 16), (1, 8)))
    mix_gate = noise(splits[3], (SEQUENCE_LENGTH, RETENTION_HEADS * HEAD_DIM), 1.0, 6.0, ((0, 16), (1, 8)))
    log_decay = draw_log_decay(jax.random.fold_in(splits[14], 71), 0)
    ret_gain = jnp.clip(1.0 + 0.18 * jax.random.normal(splits[5], (RETENTION_HEADS * HEAD_DIM,), jnp.float32), 0.1, 1.9)
    w_out = noise(splits[6], (RETENTION_HEADS * HEAD_DIM, D), (RETENTION_HEADS * HEAD_DIM) ** -0.5, 0.125)
    moe_in = noise(splits[7], (MOE_TOK, D), 1.0, 6.0, ((0, 128),))
    route_ids = draw_route_ids(jax.random.fold_in(splits[14], 71), 0)
    route_weights = jnp.clip(0.1 + 0.9 * jax.random.uniform(splits[9], (MOE_TOK, TOP), jnp.float32) ** steps_of(splits[9], (MOE_TOK, TOP), ((0, 128),), -0.2, 0.2), 0.1, 1.0)
    moe_gain = jnp.clip(1.0 + 0.18 * jax.random.normal(splits[10], (D,), jnp.float32), 0.1, 1.9)
    w_gate = noise(splits[11], (EXPERTS, D, FF), D ** -0.5, 0.125, ((0, 16), (2, 8)))
    w_up = noise(splits[12], (EXPERTS, D, FF), D ** -0.5, 0.125, ((0, 16), (2, 8)))
    w_down = noise(splits[13], (EXPERTS, FF, D), FF ** -0.5, 0.0625, ((0, 16), (1, 8)))
    return dict(mix_query=mix_query, mix_key=mix_key, mix_value=mix_value, mix_gate=mix_gate, log_decay=log_decay, ret_gain=ret_gain, w_out=w_out, moe_in=moe_in, route_ids=route_ids, route_weights=route_weights, moe_gain=moe_gain, w_gate=w_gate, w_up=w_up, w_down=w_down)


norm_eps = 1e-06

def rotate(tensor, position_index):
    head_dim = tensor.shape[-1]
    half_dim = head_dim // 2
    inverse = 10000.0 ** (-(jnp.arange(half_dim, dtype=jnp.float32) * 2.0) / head_dim)
    angle = position_index.astype(jnp.float32)[:, None] * inverse[None, :]
    cosine = jnp.cos(angle)[:, None, :]
    sine = jnp.sin(angle)[:, None, :]
    front = tensor[..., :half_dim]
    back = tensor[..., half_dim:]
    return jnp.concatenate([front * cosine - back * sine, back * cosine + front * sine], axis=-1)

def retention_blocks(query_rot, key_rot, values, log_decay):
    length = query_rot.shape[0]
    block_count = length // BLOCK
    query_blocks = query_rot.reshape(block_count, BLOCK, RETENTION_HEADS, HEAD_DIM)
    key_blocks = key_rot.reshape(block_count, BLOCK, RETENTION_HEADS, HEAD_DIM)
    value_blocks = values.reshape(block_count, BLOCK, RETENTION_HEADS, HEAD_DIM)
    cumulative = jnp.cumsum(log_decay.reshape(block_count, BLOCK, RETENTION_HEADS), axis=1)
    causal = jnp.arange(BLOCK)[:, None] >= jnp.arange(BLOCK)[None, :]

    def advance(carried, block_items):
        query_now, key_now, value_now, cumul_now = block_items
        scores = jnp.einsum('ihd,jhd->hij', query_now.astype(jnp.float32), key_now.astype(jnp.float32))
        by_head = cumul_now.T
        log_gap = by_head[:, :, None] - by_head[:, None, :]
        decay_mask = jnp.where(causal[None], jnp.exp(jnp.where(causal[None], log_gap, 0.0)), 0.0)
        weights = (scores * decay_mask).astype(jnp.bfloat16)
        within_block = jnp.einsum('hij,jhe->ihe', weights.astype(jnp.float32), value_now.astype(jnp.float32))
        block_last = cumul_now[-1]
        query_decayed = query_now.astype(jnp.float32) * jnp.exp(cumul_now)[:, :, None]
        carried_part = jnp.einsum('ihd,hde->ihe', query_decayed, carried, precision=lax.Precision.HIGHEST)
        key_decayed = (key_now.astype(jnp.float32) * jnp.exp(block_last[None, :] - cumul_now)[:, :, None]).astype(jnp.bfloat16)
        update = jnp.einsum('jhd,jhe->hde', key_decayed.astype(jnp.float32), value_now.astype(jnp.float32))
        return (jnp.exp(block_last)[:, None, None] * carried + update, within_block + carried_part)
    initial = jnp.zeros((RETENTION_HEADS, HEAD_DIM, HEAD_DIM), jnp.float32)
    final_state, outputs = lax.scan(advance, initial, (query_blocks, key_blocks, value_blocks, cumulative))
    return outputs.reshape(length, RETENTION_HEADS, HEAD_DIM)

def mixer_reference(mix_query, mix_key, mix_value, mix_gate, log_decay, ret_gain, w_out):
    length = mix_query.shape[0]
    position_index = jnp.arange(length, dtype=jnp.int32)
    query_rot = rotate(mix_query.astype(jnp.float32).reshape(length, RETENTION_HEADS, HEAD_DIM), position_index).astype(jnp.bfloat16)
    key_rot = (rotate(mix_key.astype(jnp.float32).reshape(length, RETENTION_HEADS, HEAD_DIM), position_index) * HEAD_DIM ** (-0.5)).astype(jnp.bfloat16)
    values = mix_value.reshape(length, RETENTION_HEADS, HEAD_DIM)
    retained = retention_blocks(query_rot, key_rot, values, log_decay)
    inverse_rms = lax.rsqrt(lax.optimization_barrier(jnp.mean(retained * retained, axis=-1, keepdims=True)) + norm_eps)
    gate_act = jax.nn.silu(mix_gate.astype(jnp.float32).reshape(length, RETENTION_HEADS, HEAD_DIM))
    heads_out = (gate_act * retained * inverse_rms * ret_gain.reshape(RETENTION_HEADS, HEAD_DIM)).astype(jnp.bfloat16)
    projected = jnp.dot(heads_out.reshape(length, RETENTION_HEADS * HEAD_DIM), w_out, preferred_element_type=jnp.float32)
    return projected.astype(jnp.bfloat16)

def expert_reference(moe_in, route_ids, route_weights, moe_gain, w_gate, w_up, w_down):
    tokens = moe_in.shape[0]
    model_width = moe_in.shape[1]
    block_count = tokens // MOE_DEV
    floats = moe_in.astype(jnp.float32)
    normed = (floats * lax.rsqrt(lax.optimization_barrier(jnp.mean(floats * floats, axis=-1, keepdims=True)) + norm_eps) * moe_gain).astype(jnp.bfloat16)
    block_ids = route_ids.reshape(block_count, MOE_DEV * TOP)
    onehot = (block_ids[:, :, None] == jnp.arange(EXPERTS, dtype=jnp.int32)[None, None, :]).astype(jnp.int32)
    slot_index = lax.optimization_barrier(jnp.sum(jnp.cumsum(onehot, axis=1) * onehot, axis=-1)) - 1
    buffer_rows = (jnp.arange(block_count, dtype=jnp.int32)[:, None] * CAP + slot_index).reshape(-1)
    token_index = (jnp.arange(block_count, dtype=jnp.int32)[:, None] * MOE_DEV + jnp.arange(MOE_DEV * TOP, dtype=jnp.int32)[None, :] // TOP).reshape(-1)
    flat_ids = block_ids.reshape(-1)
    buffer = jnp.zeros((EXPERTS, block_count * CAP, model_width), jnp.bfloat16)
    buffer = buffer.at[flat_ids, buffer_rows].set(normed[token_index])
    group_width = FF // N_TP

    def one_expert(expert_items):
        row_block, gate_weight, up_weight, down_weight = expert_items
        gate_part = jnp.dot(row_block, gate_weight, preferred_element_type=jnp.float32)
        up_part = jnp.dot(row_block, up_weight, preferred_element_type=jnp.float32)
        hidden = (jax.nn.silu(gate_part) * up_part).astype(jnp.bfloat16)
        summed = jnp.zeros((row_block.shape[0], model_width), jnp.float32)
        for group in range(N_TP):
            partial_value = jnp.dot(hidden[:, group * group_width:(group + 1) * group_width], down_weight[group * group_width:(group + 1) * group_width], preferred_element_type=jnp.float32).astype(jnp.bfloat16)
            summed = summed + partial_value.astype(jnp.float32)
        return summed.astype(jnp.bfloat16)
    outputs = lax.map(one_expert, (buffer, w_gate, w_up, w_down))
    picked = outputs[flat_ids, buffer_rows].reshape(tokens, TOP, model_width)
    combined = lax.optimization_barrier(jnp.sum(picked.astype(jnp.float32) * route_weights[:, :, None], axis=1))
    return combined.astype(jnp.bfloat16)

def reference(mix_query, mix_key, mix_value, mix_gate, log_decay, ret_gain, w_out, moe_in, route_ids, route_weights, moe_gain, w_gate, w_up, w_down):
    mix_out = mixer_reference(mix_query, mix_key, mix_value, mix_gate, log_decay, ret_gain, w_out)
    moe_out = expert_reference(moe_in, route_ids, route_weights, moe_gain, w_gate, w_up, w_down)
    return (mix_out, moe_out)
```

```python
import functools

import jax
import jax.numpy as jnp
import numpy as np
from jax import lax
from jax.experimental import pallas as pl
from jax.experimental.pallas import tpu as pltpu
from jax.sharding import Mesh
from jax.sharding import PartitionSpec as P

HEAD_DIM = 256
HALF = HEAD_DIM // 2
BLOCK = 512
EXPERTS = 16
CAP = 8
SLOTS = EXPERTS * CAP
norm_eps = 1e-06

f32 = jnp.float32
bf16 = jnp.bfloat16

NT = (((1,), (1,)), ((), ()))
TN = (((0,), (0,)), ((), ()))


def mm(a, b):
    return jnp.dot(a, b, preferred_element_type=f32)


def shift(x, axis, by, size=4, wrap=True):
    pairs = [(j, (j + by) % size) for j in range(size) if wrap or 0 <= j + by < size]
    return lax.ppermute(x, axis, pairs)


def route_tables(ids):
    tokens = ids.shape[0]
    lane = lax.broadcasted_iota(jnp.int32, (tokens, EXPERTS), 1)
    first = (ids[:, 0:1] == lane).astype(f32)
    second = (ids[:, 1:2] == lane).astype(f32)
    both = first + second
    below = (
        lax.broadcasted_iota(jnp.int32, (tokens, tokens), 1)
        < lax.broadcasted_iota(jnp.int32, (tokens, tokens), 0)
    ).astype(f32)
    rank = mm(below, both)
    return first, second, both, rank


def pre_kernel(x_ref, ids_ref, gain_ref, out_ref):
    _, _, both, rank = route_tables(ids_ref[...])
    tokens = x_ref.shape[0]
    row = lax.broadcasted_iota(jnp.int32, (SLOTS, EXPERTS), 0)
    col = lax.broadcasted_iota(jnp.int32, (SLOTS, EXPERTS), 1)
    spread = (row // CAP == col).astype(f32)
    named = lax.dot_general(spread, both, NT, preferred_element_type=f32)
    ranks = lax.dot_general(spread, rank, NT, preferred_element_type=f32)
    slot = (lax.broadcasted_iota(jnp.int32, (SLOTS, tokens), 0) % CAP).astype(f32)
    pick = jnp.where((named > 0.5) & (jnp.abs(ranks - slot) < 0.5), 1.0, 0.0).astype(bf16)
    x = x_ref[...].astype(f32)
    scale = lax.rsqrt(jnp.mean(x * x, axis=-1, keepdims=True) + norm_eps)
    normed = (x * scale * gain_ref[...]).astype(bf16)
    out_ref[...] = mm(pick, normed).astype(bf16)


def combine_kernel(rows_ref, ids_ref, weights_ref, out_ref):
    first, second, _, rank = route_tables(ids_ref[...])
    tokens = ids_ref.shape[0]
    row = lax.broadcasted_iota(jnp.int32, (EXPERTS, SLOTS), 0)
    col = lax.broadcasted_iota(jnp.int32, (EXPERTS, SLOTS), 1)
    spread = (col // CAP == row).astype(f32)
    slot = (lax.broadcasted_iota(jnp.int32, (tokens, SLOTS), 1) % CAP).astype(f32)
    here = jnp.abs(mm(rank, spread) - slot) < 0.5
    rows = rows_ref[...]
    total = None
    for k, named in enumerate((first, second)):
        pick = jnp.where((mm(named, spread) > 0.5) & here, 1.0, 0.0).astype(bf16)
        part = mm(pick, rows) * weights_ref[:, k : k + 1]
        total = part if total is None else total + part
    out_ref[...] = total.astype(bf16)


def ffn_kernel(n_x, tile, *refs):
    xs = refs[:n_x]
    wg, wu, wd = refs[n_x : n_x + 3]
    outs = refs[n_x + 3 : -9]
    xbuf, gbuf, ubuf, dbuf, hbuf, obuf, xsem, wsem, osem = refs[-9:]
    ff = gbuf.shape[1]
    chunks = ff // 128
    per_out = n_x // len(outs)
    copies_w = []
    for j in range(chunks):
        cols = pl.ds(j * 128, 128)
        a = pltpu.make_async_copy(wg.at[:, cols], gbuf.at[:, cols], wsem.at[2 * j])
        b = pltpu.make_async_copy(wu.at[:, cols], ubuf.at[:, cols], wsem.at[2 * j + 1])
        copies_w.append((a, b))
    for c in copies_w[0]:
        c.start()
    copies_x = []
    for i in range(n_x):
        c = pltpu.make_async_copy(xs[i], xbuf.at[pl.ds(i * tile, tile)], xsem.at[i])
        c.start()
        copies_x.append(c)
    for pair in copies_w[1:]:
        for c in pair:
            c.start()
    down = pltpu.make_async_copy(wd, dbuf, wsem.at[2 * chunks])
    down.start()
    for j in range(chunks):
        for c in copies_w[j]:
            c.wait()
        w = jnp.concatenate(
            [gbuf[:, j * 128 : (j + 1) * 128], ubuf[:, j * 128 : (j + 1) * 128]], axis=1
        )
        step = 256
        for r in range(0, n_x * tile, step):
            if j == 0:
                for i in range(r // tile, (r + step) // tile):
                    copies_x[i].wait()
            both = mm(xbuf[r : r + step, :], w)
            gate, up = both[:, :128], both[:, 128:]
            hidden = gate * up / (1.0 + jnp.exp(-gate))
            hbuf[r : r + step, j * 128 : (j + 1) * 128] = hidden.astype(bf16)
    down.wait()
    outs_c = []
    for o in range(len(outs)):
        for i in range(per_out):
            r = (o * per_out + i) * tile
            if r % 256 == 0:
                obuf[r : r + 256, :] = mm(hbuf[r : r + 256, :], dbuf[...]).astype(bf16)
                last = pltpu.make_async_copy(
                    obuf.at[pl.ds(r, 256)], outs[o].at[pl.ds(i * tile, 256)], osem.at[r // 256]
                )
                last.start()
                outs_c.append(last)
    for c in outs_c:
        c.wait()


def ffn(xs, w_gate, w_up, w_down, n_out):
    n_x = len(xs)
    tile, width = xs[0].shape
    ff = w_gate.shape[1]
    rows = n_x * tile
    hbm = pl.BlockSpec(memory_space=pl.ANY)
    return pl.pallas_call(
        functools.partial(ffn_kernel, n_x, tile),
        out_shape=[jax.ShapeDtypeStruct((rows // n_out, width), bf16)] * n_out,
        in_specs=[hbm] * (n_x + 3),
        out_specs=[hbm] * n_out,
        scratch_shapes=[
            pltpu.VMEM((rows, width), bf16),
            pltpu.VMEM((width, ff), bf16),
            pltpu.VMEM((width, ff), bf16),
            pltpu.VMEM((ff, width), bf16),
            pltpu.VMEM((rows, ff), bf16),
            pltpu.VMEM((rows, width), bf16),
            pltpu.SemaphoreType.DMA((n_x,)),
            pltpu.SemaphoreType.DMA((2 * (ff // 128) + 1,)),
            pltpu.SemaphoreType.DMA((rows // 256,)),
        ],
        cost_estimate=pl.CostEstimate(
            flops=6 * rows * width * ff,
            bytes_accessed=2 * (3 * width * ff + 2 * rows * width),
            transcendentals=rows * ff,
        ),
        name="ffn",
    )(*xs, w_gate, w_up, w_down)


def local_kernel(
    base_ref, q_ref, k_ref, v_ref, ld_ref, cos_ref, sin_ref, kept_ref, qd_ref, send_ref, state, before
):
    b = pl.program_id(0)

    @pl.when(b == 0)
    def _():
        state[...] = jnp.zeros_like(state)
        before[...] = jnp.zeros_like(before)

    cos_base = base_ref[0, 0:1, :]
    sin_base = base_ref[0, 1:2, :]
    cos_t, sin_t = cos_ref[...], sin_ref[...]
    cosine = cos_t * cos_base - sin_t * sin_base
    sine = sin_t * cos_base + cos_t * sin_base

    def rotated(ref):
        front = ref[:, :HALF].astype(f32)
        back = ref[:, HALF:].astype(f32)
        return jnp.concatenate([front * cosine - back * sine, back * cosine + front * sine], axis=1)

    q = rotated(q_ref).astype(bf16)
    k = (rotated(k_ref) * HEAD_DIM ** (-0.5)).astype(bf16)
    v = v_ref[...]
    row = lax.broadcasted_iota(jnp.int32, (BLOCK, BLOCK), 0)
    col = lax.broadcasted_iota(jnp.int32, (BLOCK, BLOCK), 1)
    ld = ld_ref[0]
    cum = jnp.sum(jnp.where(row >= col, ld, 0.0), axis=1, keepdims=True)
    cum_row = jnp.sum(jnp.where(row == col, cum, 0.0), axis=0, keepdims=True)
    last = cum[BLOCK - 1 : BLOCK, :]

    q32 = q.astype(f32)
    begin = state[...].astype(bf16)
    carried = mm((q32 * jnp.exp(cum)).astype(bf16), begin)
    half = BLOCK // 2
    for r in range(2):
        lo, hi = r * half, (r + 1) * half
        scores = lax.dot_general(q[lo:hi], k[:hi], NT, preferred_element_type=f32)
        gap = cum[lo:hi] - cum_row[:, :hi]
        seen = (
            lax.broadcasted_iota(jnp.int32, (half, hi), 0) + lo
            >= lax.broadcasted_iota(jnp.int32, (half, hi), 1)
        )
        weights = jnp.where(seen, scores * jnp.exp(jnp.where(seen, gap, 0.0)), 0.0).astype(bf16)
        kept_ref[lo:hi, :] = mm(weights, v[:hi]) + carried[lo:hi]
    qd_ref[...] = (q32 * jnp.exp(cum + before[0:1, 0:1])).astype(bf16)
    kd = (k.astype(f32) * jnp.exp(last - cum)).astype(bf16)
    update = lax.dot_general(kd, v, TN, preferred_element_type=f32)
    state[...] = jnp.exp(last) * state[...] + update
    before[...] = before[...] + last

    @pl.when(b == pl.num_programs(0) - 1)
    def _():
        send_ref[0:HEAD_DIM, :] = state[...].astype(bf16)
        put_decay(send_ref, jnp.exp(before[...]))


def put_decay(ref, decay):
    high = decay.astype(bf16)
    low = (decay - high.astype(f32)).astype(bf16)
    ref[HEAD_DIM : HEAD_DIM + 8, :HALF] = jnp.broadcast_to(high, (8, HALF))
    ref[HEAD_DIM : HEAD_DIM + 8, HALF:] = jnp.broadcast_to(low, (8, HALF))


def get_decay(ref):
    tail = ref[HEAD_DIM : HEAD_DIM + 8, :].astype(f32)
    return tail[0:1, 0:1] + tail[0:1, HALF : HALF + 1]


def local_part(base, q, k, v, ld, cos_t, sin_t):
    rows = q.shape[0]
    blocks = rows // BLOCK
    seq = pl.BlockSpec((BLOCK, HEAD_DIM), lambda b: (b, 0))
    table = pl.BlockSpec((BLOCK, HALF), lambda b: (0, 0))
    return pl.pallas_call(
        local_kernel,
        grid=(blocks,),
        out_shape=[
            jax.ShapeDtypeStruct((rows, HEAD_DIM), f32),
            jax.ShapeDtypeStruct((rows, HEAD_DIM), bf16),
            jax.ShapeDtypeStruct((HEAD_DIM + 8, HEAD_DIM), bf16),
        ],
        in_specs=[
            pl.BlockSpec((1, 2, HALF), lambda b: (b, 0, 0)),
            seq,
            seq,
            seq,
            pl.BlockSpec((1, 1, BLOCK), lambda b: (b, 0, 0)),
            table,
            table,
        ],
        out_specs=[seq, seq, pl.BlockSpec((HEAD_DIM + 8, HEAD_DIM), lambda b: (0, 0))],
        scratch_shapes=[pltpu.VMEM((HEAD_DIM, HEAD_DIM), f32), pltpu.VMEM((8, HALF), f32)],
        compiler_params=pltpu.CompilerParams(dimension_semantics=("arbitrary",)),
        cost_estimate=pl.CostEstimate(
            flops=6 * 10**9, bytes_accessed=6 * 2**20, transcendentals=2**20
        ),
        name="local",
    )(base, q, k, v, ld, cos_t, sin_t)


def middle_kernel(x_ref, own_ref, one_ref, two_ref, three_ref, before_ref, send_ref):
    x = x_ref[0]
    refs = (own_ref, one_ref, two_ref, three_ref)
    place = [lax.rem(x - s + 4, 4) for s in range(4)]
    decay = [get_decay(r) for r in refs]
    into = jnp.zeros((HEAD_DIM, HEAD_DIM), f32)
    whole = jnp.zeros((HEAD_DIM, HEAD_DIM), f32)
    through = jnp.ones((1, 1), f32)
    for s in range(4):
        after_all = jnp.ones((1, 1), f32)
        for o in range(4):
            if o != s:
                after_all = after_all * jnp.where(place[o] > place[s], decay[o], 1.0)
        part = refs[s][0:HEAD_DIM, :].astype(f32)
        whole = whole + part * after_all
        if s:
            into = into + jnp.where(s <= x, through, 0.0) * part
            through = through * jnp.where(s <= x, decay[s], 1.0)
    before_ref[0:HEAD_DIM, :] = into
    before_ref[HEAD_DIM : HEAD_DIM + 8, :] = jnp.broadcast_to(through, (8, HEAD_DIM))
    send_ref[0:HEAD_DIM, :] = whole.astype(bf16)
    total = decay[0] * decay[1] * decay[2] * decay[3]
    put_decay(send_ref, jnp.broadcast_to(total, (8, HALF)))


def middle(x, own, one, two, three):
    return pl.pallas_call(
        middle_kernel,
        out_shape=[
            jax.ShapeDtypeStruct((HEAD_DIM + 8, HEAD_DIM), f32),
            jax.ShapeDtypeStruct((HEAD_DIM + 8, HEAD_DIM), bf16),
        ],
        in_specs=[pl.BlockSpec(memory_space=pltpu.SMEM)]
        + [pl.BlockSpec(memory_space=pltpu.VMEM)] * 4,
        out_specs=[pl.BlockSpec(memory_space=pltpu.VMEM)] * 2,
        cost_estimate=pl.CostEstimate(
            flops=5 * 10**8, bytes_accessed=10**6, transcendentals=0
        ),
        name="middle",
    )(x, own, one, two, three)


def finish_kernel(
    before_ref, one_ref, two_ref, three_ref, kept_ref, qd_ref, gate_ref, gain_ref, out_ref, start
):
    @pl.when(pl.program_id(0) == 0)
    def _():
        into = three_ref[0:HEAD_DIM, :].astype(f32)
        for ref in (two_ref, one_ref):
            into = ref[0:HEAD_DIM, :].astype(f32) + get_decay(ref) * into
        through = before_ref[HEAD_DIM : HEAD_DIM + 1, 0:1]
        start[...] = (before_ref[0:HEAD_DIM, :] + through * into).astype(bf16)

    retained = kept_ref[...] + mm(qd_ref[...], start[...])
    scale = lax.rsqrt(jnp.mean(retained * retained, axis=-1, keepdims=True) + norm_eps)
    gate = gate_ref[...].astype(f32)
    gate = gate / (1.0 + jnp.exp(-gate))
    out_ref[...] = (gate * retained * scale * gain_ref[...]).astype(bf16)


def finish(before, one, two, three, kept, qd, gate, gain):
    rows = qd.shape[0]
    seq = pl.BlockSpec((BLOCK, HEAD_DIM), lambda b: (b, 0))
    whole = pl.BlockSpec((HEAD_DIM + 8, HEAD_DIM), lambda b: (0, 0))
    return pl.pallas_call(
        finish_kernel,
        grid=(rows // BLOCK,),
        out_shape=jax.ShapeDtypeStruct((rows, HEAD_DIM), bf16),
        in_specs=[whole] * 4 + [seq] * 3 + [pl.BlockSpec((1, HEAD_DIM), lambda b: (0, 0))],
        out_specs=seq,
        scratch_shapes=[pltpu.VMEM((HEAD_DIM, HEAD_DIM), bf16)],
        compiler_params=pltpu.CompilerParams(dimension_semantics=("arbitrary",)),
        cost_estimate=pl.CostEstimate(
            flops=2 * 10**9, bytes_accessed=5 * 2**20, transcendentals=2**19
        ),
        name="finish",
    )(before, one, two, three, kept, qd, gate, gain)


def project_kernel(rows_ref, w_ref, out_ref, acc):
    s = pl.program_id(0)
    part = mm(rows_ref[...], w_ref[...])

    @pl.when(s == 0)
    def _():
        acc[...] = part

    @pl.when(s > 0)
    def _():
        acc[...] = acc[...] + part

    @pl.when(s == pl.num_programs(0) - 1)
    def _():
        out_ref[...] = acc[...].astype(bf16)


def project(pieces, w_out):
    parts = 8
    rows = pieces.shape[0] // parts
    width = w_out.shape[1]
    return pl.pallas_call(
        project_kernel,
        grid=(parts,),
        out_shape=jax.ShapeDtypeStruct((rows, width), bf16),
        in_specs=[
            pl.BlockSpec((rows, HEAD_DIM), lambda s: (s, 0)),
            pl.BlockSpec((HEAD_DIM, width), lambda s: (s, 0)),
        ],
        out_specs=pl.BlockSpec((rows, width), lambda s: (0, 0)),
        scratch_shapes=[pltpu.VMEM((rows, width), f32)],
        compiler_params=pltpu.CompilerParams(dimension_semantics=("arbitrary",)),
        cost_estimate=pl.CostEstimate(
            flops=4 * 10**9, bytes_accessed=10 * 2**20, transcendentals=0
        ),
        name="project",
    )(pieces, w_out)


def angle_tables():
    inverse = 10000.0 ** (-np.arange(HALF) * 2.0 / HEAD_DIM)
    angle = np.arange(BLOCK)[:, None] * inverse[None, :]
    return np.cos(angle).astype(np.float32), np.sin(angle).astype(np.float32)


def on_device(
    mix_query,
    mix_key,
    mix_value,
    mix_gate,
    log_decay,
    ret_gain,
    w_out,
    moe_in,
    route_ids,
    route_weights,
    moe_gain,
    w_gate,
    w_up,
    w_down,
):
    seq_rows = mix_query.shape[0]
    blocks = seq_rows // BLOCK
    width = moe_in.shape[1]
    ep = ("z", "x")
    tp = ("y", "core")

    outgoing = pl.pallas_call(
        pre_kernel,
        out_shape=jax.ShapeDtypeStruct((SLOTS, width), bf16),
        cost_estimate=pl.CostEstimate(flops=2 * 10**9, bytes_accessed=10**6, transcendentals=0),
        name="pre",
    )(moe_in, route_ids, moe_gain.reshape(1, -1))
    own = lax.all_to_all(outgoing, ep, split_axis=0, concat_axis=0, tiled=True)

    cos_t, sin_t = angle_tables()
    inverse = 10000.0 ** (-np.arange(HALF) * 2.0 / HEAD_DIM)
    first = lax.axis_index(ep) * seq_rows + BLOCK * jnp.arange(blocks, dtype=jnp.int32)
    angle = first.astype(f32)[:, None] * jnp.asarray(inverse, f32)[None, :]
    base = jnp.stack([jnp.cos(angle), jnp.sin(angle)], axis=1)
    kept, qd, end = local_part(
        base,
        mix_query,
        mix_key,
        mix_value,
        log_decay.reshape(blocks, 1, BLOCK),
        jnp.asarray(cos_t),
        jnp.asarray(sin_t),
    )
    by_x = [shift(end, "x", s) for s in (1, 2, 3)]
    x_index = lax.axis_index("x").astype(jnp.int32).reshape(1)
    before, whole = middle(x_index, end, *by_x)
    by_z = [shift(whole, "z", s, wrap=False) for s in (1, 2, 3)]
    heads_out = finish(before, *by_z, kept, qd, mix_gate, ret_gain.reshape(1, -1))
    pieces = lax.all_to_all(heads_out, tp, split_axis=0, concat_axis=0, tiled=True)

    half = own.shape[0] // 2
    up1 = shift(own, "y", 1)
    down1 = shift(own, "y", -1)
    far = jnp.concatenate([shift(up1[:half], "y", 1), shift(down1[half:], "y", -1)], axis=0)
    mine = [own, up1, down1, far]
    other = [shift(v, "core", 1, 2) for v in mine]
    keep, give = ffn(mine + other, w_gate[0], w_up[0], w_down[0], 2)
    got = shift(give, "core", 1, 2)
    sums = (keep.astype(f32) + got.astype(f32)).astype(bf16)
    n = own.shape[0]
    back = [
        sums[:n],
        shift(sums[n : 2 * n], "y", -1),
        shift(sums[2 * n : 3 * n], "y", 1),
        shift(sums[3 * n :], "y", 2),
    ]
    expert_rows = sum(v.astype(f32) for v in back).astype(bf16)
    returned = lax.all_to_all(expert_rows, ep, split_axis=0, concat_axis=0, tiled=True)
    mix_out = project(pieces, w_out)
    moe_out = pl.pallas_call(
        combine_kernel,
        out_shape=jax.ShapeDtypeStruct(moe_in.shape, bf16),
        cost_estimate=pl.CostEstimate(flops=10**9, bytes_accessed=10**6, transcendentals=0),
        name="combine",
    )(returned, route_ids, route_weights)
    return (mix_out, moe_out)


def solution(mesh):
    ep, tp = ("z", "x"), ("y", "core")
    every = ep + tp
    fine = Mesh(mesh.devices.reshape(4, 4, 4, 2), every)
    in_specs = (
        P(ep, tp),
        P(ep, tp),
        P(ep, tp),
        P(ep, tp),
        P(ep, tp),
        P(tp),
        P(),
        P(every, None),
        P(every, None),
        P(every, None),
        P(),
        P(ep, None, tp),
        P(ep, None, tp),
        P(ep, tp, None),
    )
    out_specs = (P(every, None), P(every, None))
    return jax.shard_map(
        on_device, mesh=fine, in_specs=in_specs, out_specs=out_specs, check_vma=False
    )
```

```python
import functools

import jax
import jax.numpy as jnp
import numpy as np
from jax import lax
from jax.experimental import pallas as pl
from jax.experimental.pallas import tpu as pltpu
from jax.sharding import Mesh
from jax.sharding import PartitionSpec as P

HEAD_DIM = 256
HALF = HEAD_DIM // 2
BLOCK = 512
EXPERTS = 16
CAP = 8
SLOTS = EXPERTS * CAP
norm_eps = 1e-06

f32 = jnp.float32
bf16 = jnp.bfloat16

NT = (((1,), (1,)), ((), ()))
TN = (((0,), (0,)), ((), ()))


def mm(a, b):
    return jnp.dot(a, b, preferred_element_type=f32)


def shift(x, axis, by, size=4, wrap=True):
    pairs = [(j, (j + by) % size) for j in range(size) if wrap or 0 <= j + by < size]
    return lax.ppermute(x, axis, pairs)


def after(x, *earlier):
    return lax.optimization_barrier((x, *earlier))[0]


def route_tables(ids_ref):
    tokens = ids_ref.shape[1]
    expert = lax.broadcasted_iota(jnp.int32, (EXPERTS, tokens), 0)
    named = [(ids_ref[k : k + 1, :] == expert).astype(f32) for k in range(2)]
    earlier = (
        lax.broadcasted_iota(jnp.int32, (tokens, tokens), 0)
        < lax.broadcasted_iota(jnp.int32, (tokens, tokens), 1)
    ).astype(f32)
    rank = mm(named[0] + named[1], earlier)
    row = lax.broadcasted_iota(jnp.int32, (SLOTS, EXPERTS), 0)
    col = lax.broadcasted_iota(jnp.int32, (SLOTS, EXPERTS), 1)
    spread = (row // CAP == col).astype(f32)
    slot = (lax.broadcasted_iota(jnp.int32, (SLOTS, tokens), 0) % CAP).astype(f32)
    here = jnp.abs(mm(spread, rank) - slot) < 0.5
    return [jnp.where((mm(spread, n) > 0.5) & here, 1.0, 0.0) for n in named]


def pre_kernel(x_ref, ids_ref, gain_ref, out_ref):
    first, second = route_tables(ids_ref)
    x = x_ref[...].astype(f32)
    scale = lax.rsqrt(jnp.mean(x * x, axis=-1, keepdims=True) + norm_eps)
    normed = (x * scale * gain_ref[...]).astype(bf16)
    out_ref[...] = mm((first + second).astype(bf16), normed).astype(bf16)


def combine_kernel(rows_ref, ids_ref, weights_ref, out_ref):
    tokens = ids_ref.shape[1]
    rows = rows_ref[...]
    diagonal = lax.broadcasted_iota(jnp.int32, (tokens, tokens), 0) == lax.broadcasted_iota(
        jnp.int32, (tokens, tokens), 1
    )
    total = None
    for k, pick in enumerate(route_tables(ids_ref)):
        weight = jnp.sum(
            jnp.where(diagonal, weights_ref[k : k + 1, :], 0.0), axis=1, keepdims=True
        )
        part = lax.dot_general(pick.astype(bf16), rows, TN, preferred_element_type=f32) * weight
        total = part if total is None else total + part
    out_ref[...] = total.astype(bf16)


def ffn_kernel(n_x, tile, groups, *refs):
    xs = refs[:n_x]
    wg, wu, wd = refs[n_x : n_x + 3]
    outs = refs[n_x + 3 : -9]
    xbuf, gbuf, ubuf, dbuf, hbuf, obuf, xsem, wsem, osem = refs[-9:]
    per_out = n_x // len(outs)
    copies_w = []
    for j, (lo, hi) in enumerate(groups):
        cols = pl.ds(lo, hi - lo)
        a = pltpu.make_async_copy(wg.at[:, cols], gbuf.at[:, cols], wsem.at[2 * j])
        b = pltpu.make_async_copy(wu.at[:, cols], ubuf.at[:, cols], wsem.at[2 * j + 1])
        copies_w.append((a, b))
    copies_x = [
        pltpu.make_async_copy(xs[i], xbuf.at[pl.ds(i * tile, tile)], xsem.at[i])
        for i in range(n_x)
    ]
    pair = 256 // tile
    for c in copies_w[0]:
        c.start()
    for c in copies_x:
        c.start()
    for c in copies_w[1]:
        c.start()
    down = pltpu.make_async_copy(wd, dbuf, wsem.at[2 * len(groups)])
    down.start()
    for j, (lo, hi) in enumerate(groups):
        for c in copies_w[j]:
            c.wait()
        for r in range(0, n_x * tile, 256):
            if j == 0:
                for i in range(r // tile, r // tile + pair):
                    copies_x[i].wait()
            x = xbuf[r : r + 256, :]
            for at in range(lo, hi, 128):
                w = jnp.concatenate([gbuf[:, at : at + 128], ubuf[:, at : at + 128]], axis=1)
                both = mm(x, w)
                gate, up = both[:, :128], both[:, 128:]
                hidden = gate * up / (1.0 + jnp.exp(-gate))
                hbuf[r : r + 256, at : at + 128] = hidden.astype(bf16)
    down.wait()
    stores = []
    for r in range(0, n_x * tile, 256):
        obuf[r : r + 256, :] = mm(hbuf[r : r + 256, :], dbuf[...]).astype(bf16)
        for i in range(r // tile, r // tile + pair):
            to = outs[i // per_out].at[pl.ds((i % per_out) * tile, tile)]
            c = pltpu.make_async_copy(obuf.at[pl.ds(i * tile, tile)], to, osem.at[i])
            c.start()
            stores.append(c)
    for c in stores:
        c.wait()


def ffn(name, xs, w_gate, w_up, w_down, n_out):
    n_x = len(xs)
    tile, width = xs[0].shape
    ff = w_gate.shape[1]
    rows = n_x * tile
    cut = 128 * ((ff // 128 + 1) // 2)
    groups = ((0, cut), (cut, ff))
    hbm = pl.BlockSpec(memory_space=pl.ANY)
    return pl.pallas_call(
        functools.partial(ffn_kernel, n_x, tile, groups),
        out_shape=[jax.ShapeDtypeStruct((rows // n_out, width), bf16)] * n_out,
        in_specs=[hbm] * (n_x + 3),
        out_specs=[hbm] * n_out,
        scratch_shapes=[
            pltpu.VMEM((rows, width), bf16),
            pltpu.VMEM((width, ff), bf16),
            pltpu.VMEM((width, ff), bf16),
            pltpu.VMEM((ff, width), bf16),
            pltpu.VMEM((rows, ff), bf16),
            pltpu.VMEM((rows, width), bf16),
            pltpu.SemaphoreType.DMA((n_x,)),
            pltpu.SemaphoreType.DMA((2 * len(groups) + 1,)),
            pltpu.SemaphoreType.DMA((n_x,)),
        ],
        cost_estimate=pl.CostEstimate(
            flops=6 * rows * width * ff,
            bytes_accessed=2 * (3 * width * ff + 2 * rows * width),
            transcendentals=rows * ff,
        ),
        name=name,
    )(*xs, w_gate, w_up, w_down)


def local_kernel(
    base_ref, q_ref, k_ref, v_ref, ld_ref, cos_ref, sin_ref, kept_ref, qd_ref, send_ref, state, before
):
    b = pl.program_id(0)

    @pl.when(b == 0)
    def _():
        state[...] = jnp.zeros_like(state)
        before[...] = jnp.zeros_like(before)

    cos_base = base_ref[0, 0:1, :]
    sin_base = base_ref[0, 1:2, :]
    cos_t, sin_t = cos_ref[...], sin_ref[...]
    cosine = cos_t * cos_base - sin_t * sin_base
    sine = sin_t * cos_base + cos_t * sin_base

    def rotated(ref):
        front = ref[:, :HALF].astype(f32)
        back = ref[:, HALF:].astype(f32)
        return jnp.concatenate([front * cosine - back * sine, back * cosine + front * sine], axis=1)

    q = rotated(q_ref).astype(bf16)
    k = (rotated(k_ref) * HEAD_DIM ** (-0.5)).astype(bf16)
    v = v_ref[...]
    row = lax.broadcasted_iota(jnp.int32, (BLOCK, BLOCK), 0)
    col = lax.broadcasted_iota(jnp.int32, (BLOCK, BLOCK), 1)
    ld = ld_ref[0]
    cum = jnp.sum(jnp.where(row >= col, ld, 0.0), axis=1, keepdims=True)
    cum_row = jnp.sum(jnp.where(row == col, cum, 0.0), axis=0, keepdims=True)
    last = cum[BLOCK - 1 : BLOCK, :]

    q32 = q.astype(f32)
    begin = state[...].astype(bf16)
    carried = mm((q32 * jnp.exp(cum)).astype(bf16), begin)
    half = BLOCK // 2
    for r in range(2):
        lo, hi = r * half, (r + 1) * half
        scores = lax.dot_general(q[lo:hi], k[:hi], NT, preferred_element_type=f32)
        gap = cum[lo:hi] - cum_row[:, :hi]
        seen = (
            lax.broadcasted_iota(jnp.int32, (half, hi), 0) + lo
            >= lax.broadcasted_iota(jnp.int32, (half, hi), 1)
        )
        weights = jnp.where(seen, scores * jnp.exp(jnp.where(seen, gap, 0.0)), 0.0).astype(bf16)
        kept_ref[lo:hi, :] = mm(weights, v[:hi]) + carried[lo:hi]
    qd_ref[...] = (q32 * jnp.exp(cum + before[0:1, 0:1])).astype(bf16)
    kd = (k.astype(f32) * jnp.exp(last - cum)).astype(bf16)
    update = lax.dot_general(kd, v, TN, preferred_element_type=f32)
    state[...] = jnp.exp(last) * state[...] + update
    before[...] = before[...] + last

    @pl.when(b == pl.num_programs(0) - 1)
    def _():
        send_ref[0:HEAD_DIM, :] = state[...].astype(bf16)
        put_decay(send_ref, jnp.exp(before[...]))


def put_decay(ref, decay):
    high = decay.astype(bf16)
    low = (decay - high.astype(f32)).astype(bf16)
    ref[HEAD_DIM : HEAD_DIM + 8, :HALF] = jnp.broadcast_to(high, (8, HALF))
    ref[HEAD_DIM : HEAD_DIM + 8, HALF:] = jnp.broadcast_to(low, (8, HALF))


def get_decay(ref):
    tail = ref[HEAD_DIM : HEAD_DIM + 8, :].astype(f32)
    return tail[0:1, 0:1] + tail[0:1, HALF : HALF + 1]


def local_part(base, q, k, v, ld, cos_t, sin_t):
    rows = q.shape[0]
    blocks = rows // BLOCK
    seq = pl.BlockSpec((BLOCK, HEAD_DIM), lambda b: (b, 0))
    table = pl.BlockSpec((BLOCK, HALF), lambda b: (0, 0))
    return pl.pallas_call(
        local_kernel,
        grid=(blocks,),
        out_shape=[
            jax.ShapeDtypeStruct((rows, HEAD_DIM), f32),
            jax.ShapeDtypeStruct((rows, HEAD_DIM), bf16),
            jax.ShapeDtypeStruct((HEAD_DIM + 8, HEAD_DIM), bf16),
        ],
        in_specs=[
            pl.BlockSpec((1, 2, HALF), lambda b: (b, 0, 0)),
            seq,
            seq,
            seq,
            pl.BlockSpec((1, 1, BLOCK), lambda b: (b, 0, 0)),
            table,
            table,
        ],
        out_specs=[seq, seq, pl.BlockSpec((HEAD_DIM + 8, HEAD_DIM), lambda b: (0, 0))],
        scratch_shapes=[pltpu.VMEM((HEAD_DIM, HEAD_DIM), f32), pltpu.VMEM((8, HALF), f32)],
        compiler_params=pltpu.CompilerParams(dimension_semantics=("arbitrary",)),
        cost_estimate=pl.CostEstimate(
            flops=6 * 10**9, bytes_accessed=6 * 2**20, transcendentals=2**20
        ),
        name="local",
    )(base, q, k, v, ld, cos_t, sin_t)


def middle_kernel(x_ref, own_ref, one_ref, two_ref, three_ref, before_ref, send_ref):
    x = x_ref[0]
    refs = (own_ref, one_ref, two_ref, three_ref)
    place = [lax.rem(x - s + 4, 4) for s in range(4)]
    decay = [get_decay(r) for r in refs]
    into = jnp.zeros((HEAD_DIM, HEAD_DIM), f32)
    whole = jnp.zeros((HEAD_DIM, HEAD_DIM), f32)
    through = jnp.ones((1, 1), f32)
    for s in range(4):
        after_all = jnp.ones((1, 1), f32)
        for o in range(4):
            if o != s:
                after_all = after_all * jnp.where(place[o] > place[s], decay[o], 1.0)
        part = refs[s][0:HEAD_DIM, :].astype(f32)
        whole = whole + part * after_all
        if s:
            into = into + jnp.where(s <= x, through, 0.0) * part
            through = through * jnp.where(s <= x, decay[s], 1.0)
    before_ref[0:HEAD_DIM, :] = into
    before_ref[HEAD_DIM : HEAD_DIM + 8, :] = jnp.broadcast_to(through, (8, HEAD_DIM))
    send_ref[0:HEAD_DIM, :] = whole.astype(bf16)
    total = decay[0] * decay[1] * decay[2] * decay[3]
    put_decay(send_ref, jnp.broadcast_to(total, (8, HALF)))


def middle(x, own, one, two, three):
    return pl.pallas_call(
        middle_kernel,
        out_shape=[
            jax.ShapeDtypeStruct((HEAD_DIM + 8, HEAD_DIM), f32),
            jax.ShapeDtypeStruct((HEAD_DIM + 8, HEAD_DIM), bf16),
        ],
        in_specs=[pl.BlockSpec(memory_space=pltpu.SMEM)]
        + [pl.BlockSpec(memory_space=pltpu.VMEM)] * 4,
        out_specs=[pl.BlockSpec(memory_space=pltpu.VMEM)] * 2,
        cost_estimate=pl.CostEstimate(
            flops=5 * 10**8, bytes_accessed=10**6, transcendentals=0
        ),
        name="middle",
    )(x, own, one, two, three)


def finish_kernel(
    before_ref, one_ref, two_ref, three_ref, kept_ref, qd_ref, gate_ref, gain_ref, out_ref, start
):
    @pl.when(pl.program_id(0) == 0)
    def _():
        into = three_ref[0:HEAD_DIM, :].astype(f32)
        for ref in (two_ref, one_ref):
            into = ref[0:HEAD_DIM, :].astype(f32) + get_decay(ref) * into
        through = before_ref[HEAD_DIM : HEAD_DIM + 1, 0:1]
        start[...] = (before_ref[0:HEAD_DIM, :] + through * into).astype(bf16)

    retained = kept_ref[...] + mm(qd_ref[...], start[...])
    scale = lax.rsqrt(jnp.mean(retained * retained, axis=-1, keepdims=True) + norm_eps)
    gate = gate_ref[...].astype(f32)
    gate = gate / (1.0 + jnp.exp(-gate))
    out_ref[...] = (gate * retained * scale * gain_ref[...]).astype(bf16)


def finish(before, one, two, three, kept, qd, gate, gain):
    rows = qd.shape[0]
    seq = pl.BlockSpec((BLOCK, HEAD_DIM), lambda b: (b, 0))
    whole = pl.BlockSpec((HEAD_DIM + 8, HEAD_DIM), lambda b: (0, 0))
    return pl.pallas_call(
        finish_kernel,
        grid=(rows // BLOCK,),
        out_shape=jax.ShapeDtypeStruct((rows, HEAD_DIM), bf16),
        in_specs=[whole] * 4 + [seq] * 3 + [pl.BlockSpec((1, HEAD_DIM), lambda b: (0, 0))],
        out_specs=seq,
        scratch_shapes=[pltpu.VMEM((HEAD_DIM, HEAD_DIM), bf16)],
        compiler_params=pltpu.CompilerParams(dimension_semantics=("arbitrary",)),
        cost_estimate=pl.CostEstimate(
            flops=2 * 10**9, bytes_accessed=5 * 2**20, transcendentals=2**19
        ),
        name="finish",
    )(before, one, two, three, kept, qd, gate, gain)


def project_kernel(rows_ref, w_ref, out_ref):
    parts = w_ref.shape[0] // HEAD_DIM
    rows = rows_ref.shape[0] // parts
    total = None
    for s in range(parts):
        at = s * HEAD_DIM
        part = mm(rows_ref[s * rows : (s + 1) * rows, :], w_ref[at : at + HEAD_DIM, :])
        total = part if total is None else total + part
    out_ref[...] = total.astype(bf16)


def project(pieces, w_out):
    whole, width = w_out.shape
    rows = pieces.shape[0] * HEAD_DIM // whole
    cols = 256
    return pl.pallas_call(
        project_kernel,
        grid=(width // cols,),
        out_shape=jax.ShapeDtypeStruct((rows, width), bf16),
        in_specs=[
            pl.BlockSpec(pieces.shape, lambda n: (0, 0)),
            pl.BlockSpec((whole, cols), lambda n: (0, n)),
        ],
        out_specs=pl.BlockSpec((rows, cols), lambda n: (0, n)),
        compiler_params=pltpu.CompilerParams(dimension_semantics=("arbitrary",)),
        cost_estimate=pl.CostEstimate(
            flops=4 * 10**9, bytes_accessed=10 * 2**20, transcendentals=0
        ),
        name="project",
    )(pieces, w_out)


def angle_tables():
    inverse = 10000.0 ** (-np.arange(HALF) * 2.0 / HEAD_DIM)
    angle = np.arange(BLOCK)[:, None] * inverse[None, :]
    return np.cos(angle).astype(np.float32), np.sin(angle).astype(np.float32)


def on_device(
    mix_query,
    mix_key,
    mix_value,
    mix_gate,
    log_decay,
    ret_gain,
    w_out,
    moe_in,
    route_ids,
    route_weights,
    moe_gain,
    w_gate,
    w_up,
    w_down,
):
    seq_rows = mix_query.shape[0]
    blocks = seq_rows // BLOCK
    width = moe_in.shape[1]
    ep = ("z", "x")
    tp = ("y", "core")

    ids = route_ids.T
    outgoing = pl.pallas_call(
        pre_kernel,
        out_shape=jax.ShapeDtypeStruct((SLOTS, width), bf16),
        cost_estimate=pl.CostEstimate(flops=2 * 10**9, bytes_accessed=10**6, transcendentals=0),
        name="pre",
    )(moe_in, ids, moe_gain.reshape(1, -1))
    own = lax.all_to_all(outgoing, ep, split_axis=0, concat_axis=0, tiled=True)

    cos_t, sin_t = angle_tables()
    inverse = 10000.0 ** (-np.arange(HALF) * 2.0 / HEAD_DIM)
    first = lax.axis_index(ep) * seq_rows + BLOCK * jnp.arange(blocks, dtype=jnp.int32)
    angle = first.astype(f32)[:, None] * jnp.asarray(inverse, f32)[None, :]
    base = jnp.stack([jnp.cos(angle), jnp.sin(angle)], axis=1)
    kept, qd, end = local_part(
        base,
        after(mix_query, outgoing),
        mix_key,
        mix_value,
        log_decay.reshape(blocks, 1, BLOCK),
        jnp.asarray(cos_t),
        jnp.asarray(sin_t),
    )
    by_x = [shift(end, "x", s) for s in (1, 2, 3)]
    own = after(own, end)

    own_c = shift(own, "core", 1, 2)
    up = shift(own, "y", 1)
    down = shift(own, "y", -1)
    far = shift(own, "y", 2)
    x_index = lax.axis_index("x").astype(jnp.int32).reshape(1)
    before, whole = middle(x_index, end, *by_x)
    by_z = [shift(whole, "z", s, wrap=False) for s in (1, 2, 3)]
    weights = (w_gate[0], w_up[0], w_down[0])
    keep0, give0 = ffn("ffn0", [after(own, whole), own_c], *weights, 2)
    got0 = shift(give0, "core", 1, 2)
    heads_out = finish(
        after(before, keep0), *by_z, kept, qd, mix_gate, ret_gain.reshape(1, -1)
    )
    pieces = lax.all_to_all(heads_out, tp, split_axis=0, concat_axis=0, tiled=True)

    up_c = shift(up, "core", 1, 2)
    down_c = shift(down, "core", 1, 2)
    keep1, give1 = ffn("ffn1", [after(up, heads_out), down, up_c, down_c], *weights, 2)
    got1 = shift(give1, "core", 1, 2)
    far_c = shift(far, "core", 1, 2)
    near = (keep1.astype(f32) + got1.astype(f32)).astype(bf16)
    n = own.shape[0]
    back_up = shift(near[:n], "y", -1)
    back_down = shift(near[n:], "y", 1)
    keep2, give2 = ffn("ffn2", [after(far, near, pieces), far_c], *weights, 2)
    got2 = shift(give2, "core", 1, 2)
    back_far = shift((keep2.astype(f32) + got2.astype(f32)).astype(bf16), "y", 2)
    parts = (keep0, got0, back_up, back_down, back_far)
    expert_rows = sum(v.astype(f32) for v in parts).astype(bf16)
    returned = lax.all_to_all(expert_rows, ep, split_axis=0, concat_axis=0, tiled=True)
    mix_out = project(pieces, w_out)
    moe_out = pl.pallas_call(
        combine_kernel,
        out_shape=jax.ShapeDtypeStruct(moe_in.shape, bf16),
        cost_estimate=pl.CostEstimate(flops=10**9, bytes_accessed=10**6, transcendentals=0),
        name="combine",
    )(returned, ids, route_weights.T)
    return (mix_out, moe_out)


def solution(mesh):
    ep, tp = ("z", "x"), ("y", "core")
    every = ep + tp
    fine = Mesh(mesh.devices.reshape(4, 4, 4, 2), every)
    in_specs = (
        P(ep, tp),
        P(ep, tp),
        P(ep, tp),
        P(ep, tp),
        P(ep, tp),
        P(tp),
        P(),
        P(every, None),
        P(every, None),
        P(every, None),
        P(),
        P(ep, None, tp),
        P(ep, None, tp),
        P(ep, tp, None),
    )
    out_specs = (P(every, None), P(every, None))
    return jax.shard_map(
        on_device, mesh=fine, in_specs=in_specs, out_specs=out_specs, check_vma=False
    )
```

```python
import functools

import jax
import jax.numpy as jnp
import numpy as np
from jax import lax
from jax.experimental import pallas as pl
from jax.experimental.pallas import tpu as pltpu
from jax.sharding import Mesh
from jax.sharding import PartitionSpec as P


HEAD_DIM = 256
HALF = HEAD_DIM // 2
BLOCK = 512
EXPERTS = 16
CAP = 8
SLOTS = EXPERTS * CAP
norm_eps = 1e-06


f32 = jnp.float32
bf16 = jnp.bfloat16

NT = (((1,), (1,)), ((), ()))
TN = (((0,), (0,)), ((), ()))


def mm(a, b):
    return jnp.dot(a, b, preferred_element_type=f32)


def shift(x, axis, by, size=4, wrap=True):
    pairs = [(j, (j + by) % size) for j in range(size) if wrap or 0 <= j + by < size]
    return lax.ppermute(x, axis, pairs)


def after(x, *earlier):
    return lax.optimization_barrier((x, *earlier))[0]


def route_tables(ids_ref):
    tokens = ids_ref.shape[1]
    expert = lax.broadcasted_iota(jnp.int32, (EXPERTS, tokens), 0)
    named = [(ids_ref[k : k + 1, :] == expert).astype(f32) for k in range(2)]
    earlier = (
        lax.broadcasted_iota(jnp.int32, (tokens, tokens), 0)
        < lax.broadcasted_iota(jnp.int32, (tokens, tokens), 1)
    ).astype(f32)
    rank = mm(named[0] + named[1], earlier)
    row = lax.broadcasted_iota(jnp.int32, (SLOTS, EXPERTS), 0)
    col = lax.broadcasted_iota(jnp.int32, (SLOTS, EXPERTS), 1)
    spread = (row // CAP == col).astype(f32)
    slot = (lax.broadcasted_iota(jnp.int32, (SLOTS, tokens), 0) % CAP).astype(f32)
    here = jnp.abs(mm(spread, rank) - slot) < 0.5
    return [jnp.where((mm(spread, n) > 0.5) & here, 1.0, 0.0) for n in named]


def pre_kernel(x_ref, ids_ref, gain_ref, out_ref):
    first, second = route_tables(ids_ref)
    x = x_ref[...].astype(f32)
    scale = lax.rsqrt(jnp.mean(x * x, axis=-1, keepdims=True) + norm_eps)
    normed = (x * scale * gain_ref[...]).astype(bf16)
    out_ref[...] = mm((first + second).astype(bf16), normed).astype(bf16)


def combine_kernel(rows_ref, ids_ref, weights_ref, out_ref):
    tokens = ids_ref.shape[1]
    rows = rows_ref[...]
    diagonal = lax.broadcasted_iota(jnp.int32, (tokens, tokens), 0) == lax.broadcasted_iota(
        jnp.int32, (tokens, tokens), 1
    )
    total = None
    for k, pick in enumerate(route_tables(ids_ref)):
        weight = jnp.sum(
            jnp.where(diagonal, weights_ref[k : k + 1, :], 0.0), axis=1, keepdims=True
        )
        part = lax.dot_general(pick.astype(bf16), rows, TN, preferred_element_type=f32) * weight
        total = part if total is None else total + part
    out_ref[...] = total.astype(bf16)


def ffn_kernel(n_x, tile, groups, *refs):
    xs = refs[:n_x]
    wg, wu, wd = refs[n_x : n_x + 3]
    outs = refs[n_x + 3 : -9]
    xbuf, gbuf, ubuf, dbuf, hbuf, obuf, xsem, wsem, osem = refs[-9:]
    per_out = n_x // len(outs)
    copies_w = []
    for j, (lo, hi) in enumerate(groups):
        cols = pl.ds(lo, hi - lo)
        a = pltpu.make_async_copy(wg.at[:, cols], gbuf.at[:, cols], wsem.at[2 * j])
        b = pltpu.make_async_copy(wu.at[:, cols], ubuf.at[:, cols], wsem.at[2 * j + 1])
        copies_w.append((a, b))
    copies_x = [
        pltpu.make_async_copy(xs[i], xbuf.at[pl.ds(i * tile, tile)], xsem.at[i])
        for i in range(n_x)
    ]
    pair = 256 // tile
    for c in copies_w[0]:
        c.start()
    for c in copies_x:
        c.start()
    for c in copies_w[1]:
        c.start()
    down = pltpu.make_async_copy(wd, dbuf, wsem.at[2 * len(groups)])
    down.start()
    for j, (lo, hi) in enumerate(groups):
        for c in copies_w[j]:
            c.wait()
        for r in range(0, n_x * tile, 256):
            if j == 0:
                for i in range(r // tile, r // tile + pair):
                    copies_x[i].wait()
            x = xbuf[r : r + 256, :]
            for at in range(lo, hi, 128):
                w = jnp.concatenate([gbuf[:, at : at + 128], ubuf[:, at : at + 128]], axis=1)
                both = mm(x, w)
                gate, up = both[:, :128], both[:, 128:]
                hidden = gate * up / (1.0 + jnp.exp(-gate))
                hbuf[r : r + 256, at : at + 128] = hidden.astype(bf16)
    down.wait()
    stores = []
    for r in range(0, n_x * tile, 256):
        obuf[r : r + 256, :] = mm(hbuf[r : r + 256, :], dbuf[...]).astype(bf16)
        for i in range(r // tile, r // tile + pair):
            to = outs[i // per_out].at[pl.ds((i % per_out) * tile, tile)]
            c = pltpu.make_async_copy(obuf.at[pl.ds(i * tile, tile)], to, osem.at[i])
            c.start()
            stores.append(c)
    for c in stores:
        c.wait()


def ffn(xs, w_gate, w_up, w_down, n_out):
    n_x = len(xs)
    tile, width = xs[0].shape
    ff = w_gate.shape[1]
    rows = n_x * tile
    cut = 128 * ((ff // 128 + 1) // 2)
    groups = ((0, cut), (cut, ff))
    hbm = pl.BlockSpec(memory_space=pl.ANY)
    return pl.pallas_call(
        functools.partial(ffn_kernel, n_x, tile, groups),
        out_shape=[jax.ShapeDtypeStruct((rows // n_out, width), bf16)] * n_out,
        in_specs=[hbm] * (n_x + 3),
        out_specs=[hbm] * n_out,
        scratch_shapes=[
            pltpu.VMEM((rows, width), bf16),
            pltpu.VMEM((width, ff), bf16),
            pltpu.VMEM((width, ff), bf16),
            pltpu.VMEM((ff, width), bf16),
            pltpu.VMEM((rows, ff), bf16),
            pltpu.VMEM((rows, width), bf16),
            pltpu.SemaphoreType.DMA((n_x,)),
            pltpu.SemaphoreType.DMA((2 * len(groups) + 1,)),
            pltpu.SemaphoreType.DMA((n_x,)),
        ],
        cost_estimate=pl.CostEstimate(
            flops=6 * rows * width * ff,
            bytes_accessed=2 * (3 * width * ff + 2 * rows * width),
            transcendentals=rows * ff,
        ),
    )(*xs, w_gate, w_up, w_down)


def local_kernel(
    base_ref, q_ref, k_ref, v_ref, ld_ref, cos_ref, sin_ref, kept_ref, qd_ref, send_ref, state, before
):
    b = pl.program_id(0)

    @pl.when(b == 0)
    def _():
        state[...] = jnp.zeros_like(state)
        before[...] = jnp.zeros_like(before)

    cos_base = base_ref[0, 0:1, :]
    sin_base = base_ref[0, 1:2, :]
    cos_t, sin_t = cos_ref[...], sin_ref[...]
    cosine = cos_t * cos_base - sin_t * sin_base
    sine = sin_t * cos_base + cos_t * sin_base

    def rotated(ref):
        front = ref[:, :HALF].astype(f32)
        back = ref[:, HALF:].astype(f32)
        return jnp.concatenate([front * cosine - back * sine, back * cosine + front * sine], axis=1)

    q = rotated(q_ref).astype(bf16)
    k = (rotated(k_ref) * HEAD_DIM ** (-0.5)).astype(bf16)
    v = v_ref[...]
    row = lax.broadcasted_iota(jnp.int32, (BLOCK, BLOCK), 0)
    col = lax.broadcasted_iota(jnp.int32, (BLOCK, BLOCK), 1)
    ld = ld_ref[0]
    cum = jnp.sum(jnp.where(row >= col, ld, 0.0), axis=1, keepdims=True)
    cum_row = jnp.sum(jnp.where(row == col, cum, 0.0), axis=0, keepdims=True)
    last = cum[BLOCK - 1 : BLOCK, :]

    q32 = q.astype(f32)
    begin = state[...].astype(bf16)
    carried = mm((q32 * jnp.exp(cum)).astype(bf16), begin)
    half = BLOCK // 2
    for r in range(2):
        lo, hi = r * half, (r + 1) * half
        scores = lax.dot_general(q[lo:hi], k[:hi], NT, preferred_element_type=f32)
        gap = cum[lo:hi] - cum_row[:, :hi]
        seen = (
            lax.broadcasted_iota(jnp.int32, (half, hi), 0) + lo
            >= lax.broadcasted_iota(jnp.int32, (half, hi), 1)
        )
        weights = jnp.where(seen, scores * jnp.exp(jnp.where(seen, gap, 0.0)), 0.0).astype(bf16)
        kept_ref[lo:hi, :] = mm(weights, v[:hi]) + carried[lo:hi]
    qd_ref[...] = (q32 * jnp.exp(cum + before[0:1, 0:1])).astype(bf16)
    kd = (k.astype(f32) * jnp.exp(last - cum)).astype(bf16)
    update = lax.dot_general(kd, v, TN, preferred_element_type=f32)
    state[...] = jnp.exp(last) * state[...] + update
    before[...] = before[...] + last

    @pl.when(b == pl.num_programs(0) - 1)
    def _():
        send_ref[0:HEAD_DIM, :] = state[...].astype(bf16)
        put_decay(send_ref, jnp.exp(before[...]))


def put_decay(ref, decay):
    high = decay.astype(bf16)
    low = (decay - high.astype(f32)).astype(bf16)
    ref[HEAD_DIM : HEAD_DIM + 8, :HALF] = jnp.broadcast_to(high, (8, HALF))
    ref[HEAD_DIM : HEAD_DIM + 8, HALF:] = jnp.broadcast_to(low, (8, HALF))


def get_decay(ref):
    tail = ref[HEAD_DIM : HEAD_DIM + 8, :].astype(f32)
    return tail[0:1, 0:1] + tail[0:1, HALF : HALF + 1]


def local_part(base, q, k, v, ld, cos_t, sin_t):
    rows = q.shape[0]
    blocks = rows // BLOCK
    seq = pl.BlockSpec((BLOCK, HEAD_DIM), lambda b: (b, 0))
    table = pl.BlockSpec((BLOCK, HALF), lambda b: (0, 0))
    return pl.pallas_call(
        local_kernel,
        grid=(blocks,),
        out_shape=[
            jax.ShapeDtypeStruct((rows, HEAD_DIM), f32),
            jax.ShapeDtypeStruct((rows, HEAD_DIM), bf16),
            jax.ShapeDtypeStruct((HEAD_DIM + 8, HEAD_DIM), bf16),
        ],
        in_specs=[
            pl.BlockSpec((1, 2, HALF), lambda b: (b, 0, 0)),
            seq,
            seq,
            seq,
            pl.BlockSpec((1, 1, BLOCK), lambda b: (b, 0, 0)),
            table,
            table,
        ],
        out_specs=[seq, seq, pl.BlockSpec((HEAD_DIM + 8, HEAD_DIM), lambda b: (0, 0))],
        scratch_shapes=[pltpu.VMEM((HEAD_DIM, HEAD_DIM), f32), pltpu.VMEM((8, HALF), f32)],
        compiler_params=pltpu.CompilerParams(dimension_semantics=("arbitrary",)),
        cost_estimate=pl.CostEstimate(
            flops=6 * 10**9, bytes_accessed=6 * 2**20, transcendentals=2**20
        ),
        name="local",
    )(base, q, k, v, ld, cos_t, sin_t)


def middle_kernel(x_ref, own_ref, one_ref, two_ref, three_ref, before_ref, send_ref):
    x = x_ref[0]
    refs = (own_ref, one_ref, two_ref, three_ref)
    place = [lax.rem(x - s + 4, 4) for s in range(4)]
    decay = [get_decay(r) for r in refs]
    into = jnp.zeros((HEAD_DIM, HEAD_DIM), f32)
    whole = jnp.zeros((HEAD_DIM, HEAD_DIM), f32)
    through = jnp.ones((1, 1), f32)
    for s in range(4):
        after_all = jnp.ones((1, 1), f32)
        for o in range(4):
            if o != s:
                after_all = after_all * jnp.where(place[o] > place[s], decay[o], 1.0)
        part = refs[s][0:HEAD_DIM, :].astype(f32)
        whole = whole + part * after_all
        if s:
            into = into + jnp.where(s <= x, through, 0.0) * part
            through = through * jnp.where(s <= x, decay[s], 1.0)
    before_ref[0:HEAD_DIM, :] = into
    before_ref[HEAD_DIM : HEAD_DIM + 8, :] = jnp.broadcast_to(through, (8, HEAD_DIM))
    send_ref[0:HEAD_DIM, :] = whole.astype(bf16)
    total = decay[0] * decay[1] * decay[2] * decay[3]
    put_decay(send_ref, jnp.broadcast_to(total, (8, HALF)))


def middle(x, own, one, two, three):
    return pl.pallas_call(
        middle_kernel,
        out_shape=[
            jax.ShapeDtypeStruct((HEAD_DIM + 8, HEAD_DIM), f32),
            jax.ShapeDtypeStruct((HEAD_DIM + 8, HEAD_DIM), bf16),
        ],
        in_specs=[pl.BlockSpec(memory_space=pltpu.SMEM)]
        + [pl.BlockSpec(memory_space=pltpu.VMEM)] * 4,
        out_specs=[pl.BlockSpec(memory_space=pltpu.VMEM)] * 2,
        cost_estimate=pl.CostEstimate(
            flops=5 * 10**8, bytes_accessed=10**6, transcendentals=0
        ),
        name="middle",
    )(x, own, one, two, three)


def finish_kernel(
    before_ref, one_ref, two_ref, three_ref, kept_ref, qd_ref, gate_ref, gain_ref, out_ref, start
):
    @pl.when(pl.program_id(0) == 0)
    def _():
        into = three_ref[0:HEAD_DIM, :].astype(f32)
        for ref in (two_ref, one_ref):
            into = ref[0:HEAD_DIM, :].astype(f32) + get_decay(ref) * into
        through = before_ref[HEAD_DIM : HEAD_DIM + 1, 0:1]
        start[...] = (before_ref[0:HEAD_DIM, :] + through * into).astype(bf16)

    retained = kept_ref[...] + mm(qd_ref[...], start[...])
    scale = lax.rsqrt(jnp.mean(retained * retained, axis=-1, keepdims=True) + norm_eps)
    gate = gate_ref[...].astype(f32)
    gate = gate / (1.0 + jnp.exp(-gate))
    out_ref[...] = (gate * retained * scale * gain_ref[...]).astype(bf16)


def finish(before, one, two, three, kept, qd, gate, gain):
    rows = qd.shape[0]
    seq = pl.BlockSpec((BLOCK, HEAD_DIM), lambda b: (b, 0))
    whole = pl.BlockSpec((HEAD_DIM + 8, HEAD_DIM), lambda b: (0, 0))
    return pl.pallas_call(
        finish_kernel,
        grid=(rows // BLOCK,),
        out_shape=jax.ShapeDtypeStruct((rows, HEAD_DIM), bf16),
        in_specs=[whole] * 4 + [seq] * 3 + [pl.BlockSpec((1, HEAD_DIM), lambda b: (0, 0))],
        out_specs=seq,
        scratch_shapes=[pltpu.VMEM((HEAD_DIM, HEAD_DIM), bf16)],
        compiler_params=pltpu.CompilerParams(dimension_semantics=("arbitrary",)),
        cost_estimate=pl.CostEstimate(
            flops=2 * 10**9, bytes_accessed=5 * 2**20, transcendentals=2**19
        ),
        name="finish",
    )(before, one, two, three, kept, qd, gate, gain)


def project_kernel(rows_ref, w_ref, out_ref):
    parts = w_ref.shape[0] // HEAD_DIM
    rows = rows_ref.shape[0] // parts
    total = None
    for s in range(parts):
        at = s * HEAD_DIM
        part = mm(rows_ref[s * rows : (s + 1) * rows, :], w_ref[at : at + HEAD_DIM, :])
        total = part if total is None else total + part
    out_ref[...] = total.astype(bf16)


def project(pieces, w_out):
    whole, width = w_out.shape
    rows = pieces.shape[0] * HEAD_DIM // whole
    cols = 256
    return pl.pallas_call(
        project_kernel,
        grid=(width // cols,),
        out_shape=jax.ShapeDtypeStruct((rows, width), bf16),
        in_specs=[
            pl.BlockSpec(pieces.shape, lambda n: (0, 0)),
            pl.BlockSpec((whole, cols), lambda n: (0, n)),
        ],
        out_specs=pl.BlockSpec((rows, cols), lambda n: (0, n)),
        compiler_params=pltpu.CompilerParams(dimension_semantics=("arbitrary",)),
        cost_estimate=pl.CostEstimate(
            flops=4 * 10**9, bytes_accessed=10 * 2**20, transcendentals=0
        ),
        name="project",
    )(pieces, w_out)


def angle_tables():
    inverse = 10000.0 ** (-np.arange(HALF) * 2.0 / HEAD_DIM)
    angle = np.arange(BLOCK)[:, None] * inverse[None, :]
    return np.cos(angle).astype(np.float32), np.sin(angle).astype(np.float32)


def on_device(
    mix_query,
    mix_key,
    mix_value,
    mix_gate,
    log_decay,
    ret_gain,
    w_out,
    moe_in,
    route_ids,
    route_weights,
    moe_gain,
    w_gate,
    w_up,
    w_down,
):
    seq_rows = mix_query.shape[0]
    blocks = seq_rows // BLOCK
    width = moe_in.shape[1]
    ep = ("z", "x")
    tp = ("y", "core")

    ids = route_ids.T
    outgoing = pl.pallas_call(
        pre_kernel,
        out_shape=jax.ShapeDtypeStruct((SLOTS, width), bf16),
        cost_estimate=pl.CostEstimate(flops=2 * 10**9, bytes_accessed=10**6, transcendentals=0),
        name="pre",
    )(moe_in, ids, moe_gain.reshape(1, -1))
    own = lax.all_to_all(outgoing, ep, split_axis=0, concat_axis=0, tiled=True)

    cos_t, sin_t = angle_tables()
    inverse = 10000.0 ** (-np.arange(HALF) * 2.0 / HEAD_DIM)
    first = lax.axis_index(ep) * seq_rows + BLOCK * jnp.arange(blocks, dtype=jnp.int32)
    angle = first.astype(f32)[:, None] * jnp.asarray(inverse, f32)[None, :]
    base = jnp.stack([jnp.cos(angle), jnp.sin(angle)], axis=1)
    kept, qd, end = local_part(
        base,
        after(mix_query, outgoing),
        mix_key,
        mix_value,
        log_decay.reshape(blocks, 1, BLOCK),
        jnp.asarray(cos_t),
        jnp.asarray(sin_t),
    )
    by_x = [shift(end, "x", s) for s in (1, 2, 3)]
    own = after(own, end)

    up = shift(own, "y", 1)
    down = shift(own, "y", -1)
    far = shift(own, "y", 2)
    own_c = shift(own, "core", 1, 2)
    x_index = lax.axis_index("x").astype(jnp.int32).reshape(1)
    before, whole = middle(x_index, end, *by_x)
    by_z = [shift(whole, "z", s, wrap=False) for s in (1, 2, 3)]
    up_c = shift(up, "core", 1, 2)
    down_c = shift(down, "core", 1, 2)
    weights = (w_gate[0], w_up[0], w_down[0])
    n = own.shape[0]
    keep1, give1 = ffn([own, up, down, own_c, up_c, down_c], *weights, 2)
    got1 = shift(give1, "core", 1, 2)
    far_c = shift(far, "core", 1, 2)
    near = (keep1.astype(f32) + got1.astype(f32)).astype(bf16)
    back_up = shift(near[n : 2 * n], "y", -1)
    back_down = shift(near[2 * n :], "y", 1)
    keep2, give2 = ffn([after(far, near), far_c], *weights, 2)
    got2 = shift(give2, "core", 1, 2)
    back_far = shift((keep2.astype(f32) + got2.astype(f32)).astype(bf16), "y", 2)
    heads_out = finish(
        before, *by_z, kept, qd, mix_gate, ret_gain.reshape(1, -1)
    )
    pieces = lax.all_to_all(heads_out, tp, split_axis=0, concat_axis=0, tiled=True)
    parts = (near[:n], back_up, back_down, back_far)
    expert_rows = sum(v.astype(f32) for v in parts).astype(bf16)
    returned = lax.all_to_all(expert_rows, ep, split_axis=0, concat_axis=0, tiled=True)
    mix_out = project(pieces, w_out)
    moe_out = pl.pallas_call(
        combine_kernel,
        out_shape=jax.ShapeDtypeStruct(moe_in.shape, bf16),
        cost_estimate=pl.CostEstimate(flops=10**9, bytes_accessed=10**6, transcendentals=0),
        name="combine",
    )(returned, ids, route_weights.T)
    return (mix_out, moe_out)


def solution(mesh):
    ep, tp = ("z", "x"), ("y", "core")
    every = ep + tp
    fine = Mesh(mesh.devices.reshape(4, 4, 4, 2), every)
    in_specs = (
        P(ep, tp),
        P(ep, tp),
        P(ep, tp),
        P(ep, tp),
        P(ep, tp),
        P(tp),
        P(),
        P(every, None),
        P(every, None),
        P(every, None),
        P(),
        P(ep, None, tp),
        P(ep, None, tp),
        P(ep, tp, None),
    )
    out_specs = (P(every, None), P(every, None))

    return jax.shard_map(
        on_device, mesh=fine, in_specs=in_specs, out_specs=out_specs, check_vma=False
    )
```

```python
import functools

import jax
import jax.numpy as jnp
import numpy as np
from jax import lax
from jax.experimental import pallas as pl
from jax.experimental.pallas import tpu as pltpu
from jax.sharding import Mesh
from jax.sharding import PartitionSpec as P


HEAD_DIM = 256
HALF = HEAD_DIM // 2
BLOCK = 512
EXPERTS = 16
CAP = 8
SLOTS = EXPERTS * CAP
norm_eps = 1e-06


FFN_VMEM = 30 * 2**20

f32 = jnp.float32
bf16 = jnp.bfloat16

NT = (((1,), (1,)), ((), ()))
TN = (((0,), (0,)), ((), ()))


def mm(a, b):
    return jnp.dot(a, b, preferred_element_type=f32)


def shift(x, axis, by, size=4, wrap=True):
    pairs = [(j, (j + by) % size) for j in range(size) if wrap or 0 <= j + by < size]
    return lax.ppermute(x, axis, pairs)


def vm(x):
    return pltpu.with_memory_space_constraint(x, pltpu.VMEM)


def after(x, *earlier):
    return lax.optimization_barrier((x, *earlier))[0]


def route_tables(ids_ref):
    tokens = ids_ref.shape[1]
    expert = lax.broadcasted_iota(jnp.int32, (EXPERTS, tokens), 0)
    named = [(ids_ref[k : k + 1, :] == expert).astype(f32) for k in range(2)]
    earlier = (
        lax.broadcasted_iota(jnp.int32, (tokens, tokens), 0)
        < lax.broadcasted_iota(jnp.int32, (tokens, tokens), 1)
    ).astype(f32)
    rank = mm(named[0] + named[1], earlier)
    row = lax.broadcasted_iota(jnp.int32, (SLOTS, EXPERTS), 0)
    col = lax.broadcasted_iota(jnp.int32, (SLOTS, EXPERTS), 1)
    spread = (row // CAP == col).astype(f32)
    slot = (lax.broadcasted_iota(jnp.int32, (SLOTS, tokens), 0) % CAP).astype(f32)
    here = jnp.abs(mm(spread, rank) - slot) < 0.5
    return [jnp.where((mm(spread, n) > 0.5) & here, 1.0, 0.0) for n in named]


def pre_kernel(x_ref, ids_ref, gain_ref, out_ref):
    first, second = route_tables(ids_ref)
    x = x_ref[...].astype(f32)
    scale = lax.rsqrt(jnp.mean(x * x, axis=-1, keepdims=True) + norm_eps)
    normed = (x * scale * gain_ref[...]).astype(bf16)
    out_ref[...] = mm((first + second).astype(bf16), normed).astype(bf16)


def combine_kernel(rows_ref, ids_ref, weights_ref, out_ref):
    tokens = ids_ref.shape[1]
    rows = rows_ref[...]
    diagonal = lax.broadcasted_iota(jnp.int32, (tokens, tokens), 0) == lax.broadcasted_iota(
        jnp.int32, (tokens, tokens), 1
    )
    total = None
    for k, pick in enumerate(route_tables(ids_ref)):
        weight = jnp.sum(
            jnp.where(diagonal, weights_ref[k : k + 1, :], 0.0), axis=1, keepdims=True
        )
        part = lax.dot_general(pick.astype(bf16), rows, TN, preferred_element_type=f32) * weight
        total = part if total is None else total + part
    out_ref[...] = total.astype(bf16)


def ffn_kernel(n_x, *refs):
    xs = refs[:n_x]
    wg, wu, wd = refs[n_x : n_x + 3]
    outs = refs[n_x + 3 : -1]
    hbuf = refs[-1]
    tile = xs[0].shape[0]
    for i in range(n_x):
        x = xs[i][...]
        for at in range(0, hbuf.shape[1], 128):
            w = jnp.concatenate([wg[:, at : at + 128], wu[:, at : at + 128]], axis=1)
            both = mm(x, w)
            gate, up = both[:, :128], both[:, 128:]
            hidden = gate * up / (1.0 + jnp.exp(-gate))
            hbuf[i * tile : (i + 1) * tile, at : at + 128] = hidden.astype(bf16)
    keep = len(outs) - 1
    for i in range(n_x):
        out = mm(hbuf[i * tile : (i + 1) * tile, :], wd[...]).astype(bf16)
        if i < keep:
            outs[i][...] = out
        else:
            at = (i - keep) * tile
            outs[keep][at : at + tile, :] = out


def ffn(keep, give, weights):
    n_x = len(keep) + len(give)
    tile, width = keep[0].shape
    ff = weights[0].shape[1]
    rows = n_x * tile
    in_vmem = pl.BlockSpec(memory_space=pltpu.VMEM)
    return pl.pallas_call(
        functools.partial(ffn_kernel, n_x),
        out_shape=[pltpu.VMEM((tile, width), bf16)] * len(keep)
        + [pltpu.VMEM((len(give) * tile, width), bf16)],
        in_specs=[in_vmem] * (n_x + 3),
        out_specs=[in_vmem] * (len(keep) + 1),
        scratch_shapes=[pltpu.VMEM((rows, ff), bf16)],
        compiler_params=pltpu.CompilerParams(vmem_limit_bytes=FFN_VMEM),
        cost_estimate=pl.CostEstimate(
            flops=6 * rows * width * ff,
            bytes_accessed=2 * (3 * width * ff + 2 * rows * width),
            transcendentals=rows * ff,
        ),
    )(*[vm(x) for x in (*keep, *give)], *[vm(w) for w in weights])


def local_kernel(
    base_ref, q_ref, k_ref, v_ref, ld_ref, cos_ref, sin_ref, kept_ref, qd_ref, send_ref, state, before
):
    b = pl.program_id(0)

    @pl.when(b == 0)
    def _():
        state[...] = jnp.zeros_like(state)
        before[...] = jnp.zeros_like(before)

    cos_base = base_ref[0, 0:1, :]
    sin_base = base_ref[0, 1:2, :]
    cos_t, sin_t = cos_ref[...], sin_ref[...]
    cosine = cos_t * cos_base - sin_t * sin_base
    sine = sin_t * cos_base + cos_t * sin_base

    def rotated(ref):
        front = ref[:, :HALF].astype(f32)
        back = ref[:, HALF:].astype(f32)
        return jnp.concatenate([front * cosine - back * sine, back * cosine + front * sine], axis=1)

    q = rotated(q_ref).astype(bf16)
    k = (rotated(k_ref) * HEAD_DIM ** (-0.5)).astype(bf16)
    v = v_ref[...]
    row = lax.broadcasted_iota(jnp.int32, (BLOCK, BLOCK), 0)
    col = lax.broadcasted_iota(jnp.int32, (BLOCK, BLOCK), 1)
    ld = ld_ref[0]
    cum = jnp.sum(jnp.where(row >= col, ld, 0.0), axis=1, keepdims=True)
    cum_row = jnp.sum(jnp.where(row == col, cum, 0.0), axis=0, keepdims=True)
    last = cum[BLOCK - 1 : BLOCK, :]

    q32 = q.astype(f32)
    begin = state[...].astype(bf16)
    carried = mm((q32 * jnp.exp(cum)).astype(bf16), begin)
    half = BLOCK // 2
    for r in range(2):
        lo, hi = r * half, (r + 1) * half
        scores = lax.dot_general(q[lo:hi], k[:hi], NT, preferred_element_type=f32)
        gap = cum[lo:hi] - cum_row[:, :hi]
        seen = (
            lax.broadcasted_iota(jnp.int32, (half, hi), 0) + lo
            >= lax.broadcasted_iota(jnp.int32, (half, hi), 1)
        )
        weights = jnp.where(seen, scores * jnp.exp(jnp.where(seen, gap, 0.0)), 0.0).astype(bf16)
        kept_ref[lo:hi, :] = mm(weights, v[:hi]) + carried[lo:hi]
    qd_ref[...] = (q32 * jnp.exp(cum + before[0:1, 0:1])).astype(bf16)
    kd = (k.astype(f32) * jnp.exp(last - cum)).astype(bf16)
    update = lax.dot_general(kd, v, TN, preferred_element_type=f32)
    state[...] = jnp.exp(last) * state[...] + update
    before[...] = before[...] + last

    @pl.when(b == pl.num_programs(0) - 1)
    def _():
        send_ref[0:HEAD_DIM, :] = state[...].astype(bf16)
        put_decay(send_ref, jnp.exp(before[...]))


def put_decay(ref, decay):
    high = decay.astype(bf16)
    low = (decay - high.astype(f32)).astype(bf16)
    ref[HEAD_DIM : HEAD_DIM + 8, :HALF] = jnp.broadcast_to(high, (8, HALF))
    ref[HEAD_DIM : HEAD_DIM + 8, HALF:] = jnp.broadcast_to(low, (8, HALF))


def get_decay(ref):
    tail = ref[HEAD_DIM : HEAD_DIM + 8, :].astype(f32)
    return tail[0:1, 0:1] + tail[0:1, HALF : HALF + 1]


def local_part(base, q, k, v, ld, cos_t, sin_t):
    rows = q.shape[0]
    blocks = rows // BLOCK
    seq = pl.BlockSpec((BLOCK, HEAD_DIM), lambda b: (b, 0))
    table = pl.BlockSpec((BLOCK, HALF), lambda b: (0, 0))
    return pl.pallas_call(
        local_kernel,
        grid=(blocks,),
        out_shape=[
            jax.ShapeDtypeStruct((rows, HEAD_DIM), f32),
            jax.ShapeDtypeStruct((rows, HEAD_DIM), bf16),
            jax.ShapeDtypeStruct((HEAD_DIM + 8, HEAD_DIM), bf16),
        ],
        in_specs=[
            pl.BlockSpec((1, 2, HALF), lambda b: (b, 0, 0)),
            seq,
            seq,
            seq,
            pl.BlockSpec((1, 1, BLOCK), lambda b: (b, 0, 0)),
            table,
            table,
        ],
        out_specs=[seq, seq, pl.BlockSpec((HEAD_DIM + 8, HEAD_DIM), lambda b: (0, 0))],
        scratch_shapes=[pltpu.VMEM((HEAD_DIM, HEAD_DIM), f32), pltpu.VMEM((8, HALF), f32)],
        compiler_params=pltpu.CompilerParams(dimension_semantics=("arbitrary",)),
        cost_estimate=pl.CostEstimate(
            flops=6 * 10**9, bytes_accessed=6 * 2**20, transcendentals=2**20
        ),
        name="local",
    )(base, q, k, v, ld, cos_t, sin_t)


def middle_kernel(x_ref, own_ref, one_ref, two_ref, three_ref, before_ref, send_ref):
    x = x_ref[0]
    refs = (own_ref, one_ref, two_ref, three_ref)
    place = [lax.rem(x - s + 4, 4) for s in range(4)]
    decay = [get_decay(r) for r in refs]
    into = jnp.zeros((HEAD_DIM, HEAD_DIM), f32)
    whole = jnp.zeros((HEAD_DIM, HEAD_DIM), f32)
    through = jnp.ones((1, 1), f32)
    for s in range(4):
        after_all = jnp.ones((1, 1), f32)
        for o in range(4):
            if o != s:
                after_all = after_all * jnp.where(place[o] > place[s], decay[o], 1.0)
        part = refs[s][0:HEAD_DIM, :].astype(f32)
        whole = whole + part * after_all
        if s:
            into = into + jnp.where(s <= x, through, 0.0) * part
            through = through * jnp.where(s <= x, decay[s], 1.0)
    before_ref[0:HEAD_DIM, :] = into
    before_ref[HEAD_DIM : HEAD_DIM + 8, :] = jnp.broadcast_to(through, (8, HEAD_DIM))
    send_ref[0:HEAD_DIM, :] = whole.astype(bf16)
    total = decay[0] * decay[1] * decay[2] * decay[3]
    put_decay(send_ref, jnp.broadcast_to(total, (8, HALF)))


def middle(x, own, one, two, three):
    return pl.pallas_call(
        middle_kernel,
        out_shape=[
            jax.ShapeDtypeStruct((HEAD_DIM + 8, HEAD_DIM), f32),
            jax.ShapeDtypeStruct((HEAD_DIM + 8, HEAD_DIM), bf16),
        ],
        in_specs=[pl.BlockSpec(memory_space=pltpu.SMEM)]
        + [pl.BlockSpec(memory_space=pltpu.VMEM)] * 4,
        out_specs=[pl.BlockSpec(memory_space=pltpu.VMEM)] * 2,
        cost_estimate=pl.CostEstimate(
            flops=5 * 10**8, bytes_accessed=10**6, transcendentals=0
        ),
        name="middle",
    )(x, own, one, two, three)


def finish_kernel(
    before_ref, one_ref, two_ref, three_ref, kept_ref, qd_ref, gate_ref, gain_ref, out_ref, start
):
    @pl.when(pl.program_id(0) == 0)
    def _():
        into = three_ref[0:HEAD_DIM, :].astype(f32)
        for ref in (two_ref, one_ref):
            into = ref[0:HEAD_DIM, :].astype(f32) + get_decay(ref) * into
        through = before_ref[HEAD_DIM : HEAD_DIM + 1, 0:1]
        start[...] = (before_ref[0:HEAD_DIM, :] + through * into).astype(bf16)

    retained = kept_ref[...] + mm(qd_ref[...], start[...])
    scale = lax.rsqrt(jnp.mean(retained * retained, axis=-1, keepdims=True) + norm_eps)
    gate = gate_ref[...].astype(f32)
    gate = gate / (1.0 + jnp.exp(-gate))
    out_ref[...] = (gate * retained * scale * gain_ref[...]).astype(bf16)


def finish(before, one, two, three, kept, qd, gate, gain):
    rows = qd.shape[0]
    seq = pl.BlockSpec((BLOCK, HEAD_DIM), lambda b: (b, 0))
    whole = pl.BlockSpec((HEAD_DIM + 8, HEAD_DIM), lambda b: (0, 0))
    return pl.pallas_call(
        finish_kernel,
        grid=(rows // BLOCK,),
        out_shape=jax.ShapeDtypeStruct((rows, HEAD_DIM), bf16),
        in_specs=[whole] * 4 + [seq] * 3 + [pl.BlockSpec((1, HEAD_DIM), lambda b: (0, 0))],
        out_specs=seq,
        scratch_shapes=[pltpu.VMEM((HEAD_DIM, HEAD_DIM), bf16)],
        compiler_params=pltpu.CompilerParams(dimension_semantics=("arbitrary",)),
        cost_estimate=pl.CostEstimate(
            flops=2 * 10**9, bytes_accessed=5 * 2**20, transcendentals=2**19
        ),
        name="finish",
    )(before, one, two, three, kept, qd, gate, gain)


def project_kernel(rows_ref, w_ref, out_ref):
    parts = w_ref.shape[0] // HEAD_DIM
    rows = rows_ref.shape[0] // parts
    total = None
    for s in range(parts):
        at = s * HEAD_DIM
        part = mm(rows_ref[s * rows : (s + 1) * rows, :], w_ref[at : at + HEAD_DIM, :])
        total = part if total is None else total + part
    out_ref[...] = total.astype(bf16)


def project(pieces, w_out):
    whole, width = w_out.shape
    rows = pieces.shape[0] * HEAD_DIM // whole
    cols = 256
    return pl.pallas_call(
        project_kernel,
        grid=(width // cols,),
        out_shape=jax.ShapeDtypeStruct((rows, width), bf16),
        in_specs=[
            pl.BlockSpec(pieces.shape, lambda n: (0, 0)),
            pl.BlockSpec((whole, cols), lambda n: (0, n)),
        ],
        out_specs=pl.BlockSpec((rows, cols), lambda n: (0, n)),
        compiler_params=pltpu.CompilerParams(dimension_semantics=("arbitrary",)),
        cost_estimate=pl.CostEstimate(
            flops=4 * 10**9, bytes_accessed=10 * 2**20, transcendentals=0
        ),
        name="project",
    )(pieces, w_out)


def angle_tables():
    inverse = 10000.0 ** (-np.arange(HALF) * 2.0 / HEAD_DIM)
    angle = np.arange(BLOCK)[:, None] * inverse[None, :]
    return np.cos(angle).astype(np.float32), np.sin(angle).astype(np.float32)


def on_device(
    mix_query,
    mix_key,
    mix_value,
    mix_gate,
    log_decay,
    ret_gain,
    w_out,
    moe_in,
    route_ids,
    route_weights,
    moe_gain,
    w_gate,
    w_up,
    w_down,
):
    seq_rows = mix_query.shape[0]
    blocks = seq_rows // BLOCK
    width = moe_in.shape[1]
    ep = ("z", "x")
    tp = ("y", "core")

    ids = route_ids.T
    outgoing = pl.pallas_call(
        pre_kernel,
        out_shape=jax.ShapeDtypeStruct((SLOTS, width), bf16),
        cost_estimate=pl.CostEstimate(flops=2 * 10**9, bytes_accessed=10**6, transcendentals=0),
        name="pre",
    )(moe_in, ids, moe_gain.reshape(1, -1))
    own = lax.all_to_all(outgoing, ep, split_axis=0, concat_axis=0, tiled=True)

    cos_t, sin_t = angle_tables()
    inverse = 10000.0 ** (-np.arange(HALF) * 2.0 / HEAD_DIM)
    first = lax.axis_index(ep) * seq_rows + BLOCK * jnp.arange(blocks, dtype=jnp.int32)
    angle = first.astype(f32)[:, None] * jnp.asarray(inverse, f32)[None, :]
    base = jnp.stack([jnp.cos(angle), jnp.sin(angle)], axis=1)
    kept, qd, end = local_part(
        base,
        after(mix_query, outgoing),
        mix_key,
        mix_value,
        log_decay.reshape(blocks, 1, BLOCK),
        jnp.asarray(cos_t),
        jnp.asarray(sin_t),
    )
    by_x = [shift(end, "x", s) for s in (1, 2, 3)]
    own = after(own, end)

    up = shift(own, "y", 1)
    down = shift(own, "y", -1)
    far = shift(own, "y", 2)
    own_c = shift(own, "core", 1, 2)
    x_index = lax.axis_index("x").astype(jnp.int32).reshape(1)
    before, whole = middle(x_index, end, *by_x)
    by_z = [shift(whole, "z", s, wrap=False) for s in (1, 2, 3)]
    up_c = shift(up, "core", 1, 2)
    down_c = shift(down, "core", 1, 2)
    weights = (w_gate[0], w_up[0], w_down[0])
    n = own.shape[0]
    *keep, give1 = ffn([own, up, down], [own_c, up_c, down_c], weights)
    got1 = shift(give1, "core", 1, 2)
    far_c = shift(far, "core", 1, 2)
    near = [
        (k.astype(f32) + got1[i * n : (i + 1) * n].astype(f32)).astype(bf16)
        for i, k in enumerate(keep)
    ]
    back_up = shift(near[1], "y", -1)
    back_down = shift(near[2], "y", 1)
    keep2, give2 = ffn([after(far, near[2])], [far_c], weights)
    got2 = shift(give2, "core", 1, 2)
    back_far = shift((keep2.astype(f32) + got2.astype(f32)).astype(bf16), "y", 2)
    heads_out = finish(
        before, *by_z, kept, qd, mix_gate, ret_gain.reshape(1, -1)
    )
    pieces = lax.all_to_all(heads_out, tp, split_axis=0, concat_axis=0, tiled=True)
    parts = (near[0], back_up, back_down, back_far)
    expert_rows = sum(v.astype(f32) for v in parts).astype(bf16)
    returned = lax.all_to_all(expert_rows, ep, split_axis=0, concat_axis=0, tiled=True)
    mix_out = project(pieces, w_out)
    moe_out = pl.pallas_call(
        combine_kernel,
        out_shape=jax.ShapeDtypeStruct(moe_in.shape, bf16),
        cost_estimate=pl.CostEstimate(flops=10**9, bytes_accessed=10**6, transcendentals=0),
        name="combine",
    )(returned, ids, route_weights.T)
    return (mix_out, moe_out)


def solution(mesh):
    ep, tp = ("z", "x"), ("y", "core")
    every = ep + tp
    fine = Mesh(mesh.devices.reshape(4, 4, 4, 2), every)
    in_specs = (
        P(ep, tp),
        P(ep, tp),
        P(ep, tp),
        P(ep, tp),
        P(ep, tp),
        P(tp),
        P(),
        P(every, None),
        P(every, None),
        P(every, None),
        P(),
        P(ep, None, tp),
        P(ep, None, tp),
        P(ep, tp, None),
    )
    out_specs = (P(every, None), P(every, None))

    return jax.shard_map(
        on_device, mesh=fine, in_specs=in_specs, out_specs=out_specs, check_vma=False
    )
```

```python
import functools

import jax
import jax.numpy as jnp
import numpy as np
from jax import lax
from jax.experimental import pallas as pl
from jax.experimental.pallas import tpu as pltpu
from jax.sharding import Mesh
from jax.sharding import PartitionSpec as P


HEAD_DIM = 256
HALF = HEAD_DIM // 2
BLOCK = 512
EXPERTS = 16
CAP = 8
SLOTS = EXPERTS * CAP
norm_eps = 1e-06


MIB = 2**20

f32 = jnp.float32
bf16 = jnp.bfloat16

NT = (((1,), (1,)), ((), ()))
TN = (((0,), (0,)), ((), ()))


def mm(a, b):
    return jnp.dot(a, b, preferred_element_type=f32)


def shift(x, axis, by, size=4, wrap=True):
    pairs = [(j, (j + by) % size) for j in range(size) if wrap or 0 <= j + by < size]
    return lax.ppermute(x, axis, pairs)


def vm(x):
    return pltpu.with_memory_space_constraint(x, pltpu.VMEM)


def grid_params(mib):
    return pltpu.CompilerParams(
        dimension_semantics=("arbitrary",), vmem_limit_bytes=mib * MIB
    )


def after(x, *earlier):
    return lax.optimization_barrier((x, *earlier))[0]


def route_tables(ids_ref):
    tokens = ids_ref.shape[1]
    expert = lax.broadcasted_iota(jnp.int32, (EXPERTS, tokens), 0)
    named = [(ids_ref[k : k + 1, :] == expert).astype(f32) for k in range(2)]
    earlier = (
        lax.broadcasted_iota(jnp.int32, (tokens, tokens), 0)
        < lax.broadcasted_iota(jnp.int32, (tokens, tokens), 1)
    ).astype(f32)
    rank = mm(named[0] + named[1], earlier)
    row = lax.broadcasted_iota(jnp.int32, (SLOTS, EXPERTS), 0)
    col = lax.broadcasted_iota(jnp.int32, (SLOTS, EXPERTS), 1)
    spread = (row // CAP == col).astype(f32)
    slot = (lax.broadcasted_iota(jnp.int32, (SLOTS, tokens), 0) % CAP).astype(f32)
    here = jnp.abs(mm(spread, rank) - slot) < 0.5
    return [jnp.where((mm(spread, n) > 0.5) & here, 1.0, 0.0) for n in named]


def pre_kernel(x_ref, ids_ref, gain_ref, out_ref):
    first, second = route_tables(ids_ref)
    x = x_ref[...].astype(f32)
    scale = lax.rsqrt(jnp.mean(x * x, axis=-1, keepdims=True) + norm_eps)
    normed = (x * scale * gain_ref[...]).astype(bf16)
    out_ref[...] = mm((first + second).astype(bf16), normed).astype(bf16)


def combine_kernel(rows_ref, ids_ref, weights_ref, out_ref):
    tokens = ids_ref.shape[1]
    rows = rows_ref[...]
    diagonal = lax.broadcasted_iota(jnp.int32, (tokens, tokens), 0) == lax.broadcasted_iota(
        jnp.int32, (tokens, tokens), 1
    )
    total = None
    for k, pick in enumerate(route_tables(ids_ref)):
        weight = jnp.sum(
            jnp.where(diagonal, weights_ref[k : k + 1, :], 0.0), axis=1, keepdims=True
        )
        part = lax.dot_general(pick.astype(bf16), rows, TN, preferred_element_type=f32) * weight
        total = part if total is None else total + part
    out_ref[...] = total.astype(bf16)


def ffn_kernel(n_x, *refs):
    xs = refs[:n_x]
    wg, wu, wd = refs[n_x : n_x + 3]
    outs = refs[n_x + 3 : -1]
    hbuf = refs[-1]
    tile = xs[0].shape[0]
    for i in range(n_x):
        x = xs[i][...]
        for at in range(0, hbuf.shape[1], 128):
            w = jnp.concatenate([wg[:, at : at + 128], wu[:, at : at + 128]], axis=1)
            both = mm(x, w)
            gate, up = both[:, :128], both[:, 128:]
            hidden = gate * up / (1.0 + jnp.exp(-gate))
            hbuf[i * tile : (i + 1) * tile, at : at + 128] = hidden.astype(bf16)
    keep = len(outs) - 1
    for i in range(n_x):
        out = mm(hbuf[i * tile : (i + 1) * tile, :], wd[...]).astype(bf16)
        if i < keep:
            outs[i][...] = out
        else:
            at = (i - keep) * tile
            outs[keep][at : at + tile, :] = out


def ffn(keep, give, weights):
    n_x = len(keep) + len(give)
    tile, width = keep[0].shape
    ff = weights[0].shape[1]
    rows = n_x * tile
    in_vmem = pl.BlockSpec(memory_space=pltpu.VMEM)
    return pl.pallas_call(
        functools.partial(ffn_kernel, n_x),
        out_shape=[pltpu.VMEM((tile, width), bf16)] * len(keep)
        + [pltpu.VMEM((len(give) * tile, width), bf16)],
        in_specs=[in_vmem] * (n_x + 3),
        out_specs=[in_vmem] * (len(keep) + 1),
        scratch_shapes=[pltpu.VMEM((rows, ff), bf16)],
        compiler_params=pltpu.CompilerParams(vmem_limit_bytes=30 * MIB),
        cost_estimate=pl.CostEstimate(
            flops=6 * rows * width * ff,
            bytes_accessed=2 * (3 * width * ff + 2 * rows * width),
            transcendentals=rows * ff,
        ),
    )(*[vm(x) for x in (*keep, *give)], *weights)


def local_kernel(
    base_ref,
    q_ref,
    k_ref,
    v_ref,
    ld_ref,
    cos_ref,
    sin_ref,
    kept_ref,
    qd_ref,
    send_ref,
    state,
    before,
):
    b = pl.program_id(0)

    @pl.when(b == 0)
    def _():
        state[...] = jnp.zeros_like(state)
        before[...] = jnp.zeros_like(before)

    cos_base = base_ref[0, 0:1, :]
    sin_base = base_ref[0, 1:2, :]
    cos_t, sin_t = cos_ref[...], sin_ref[...]
    cosine = cos_t * cos_base - sin_t * sin_base
    sine = sin_t * cos_base + cos_t * sin_base

    def rotated(ref):
        front = ref[:, :HALF].astype(f32)
        back = ref[:, HALF:].astype(f32)
        return jnp.concatenate([front * cosine - back * sine, back * cosine + front * sine], axis=1)

    q = rotated(q_ref).astype(bf16)
    k = (rotated(k_ref) * HEAD_DIM ** (-0.5)).astype(bf16)
    v = v_ref[...]
    row = lax.broadcasted_iota(jnp.int32, (BLOCK, BLOCK), 0)
    col = lax.broadcasted_iota(jnp.int32, (BLOCK, BLOCK), 1)
    ld = ld_ref[0]
    cum = jnp.sum(jnp.where(row >= col, ld, 0.0), axis=1, keepdims=True)
    cum_row = jnp.sum(jnp.where(row == col, cum, 0.0), axis=0, keepdims=True)
    last = cum[BLOCK - 1 : BLOCK, :]

    q32 = q.astype(f32)
    begin = state[...].astype(bf16)
    carried = mm((q32 * jnp.exp(cum)).astype(bf16), begin)
    half = BLOCK // 2
    for r in range(2):
        lo, hi = r * half, (r + 1) * half
        scores = lax.dot_general(q[lo:hi], k[:hi], NT, preferred_element_type=f32)
        gap = cum[lo:hi] - cum_row[:, :hi]
        seen = (
            lax.broadcasted_iota(jnp.int32, (half, hi), 0) + lo
            >= lax.broadcasted_iota(jnp.int32, (half, hi), 1)
        )
        weights = jnp.where(seen, scores * jnp.exp(jnp.where(seen, gap, 0.0)), 0.0).astype(bf16)
        kept_ref[lo:hi, :] = mm(weights, v[:hi]) + carried[lo:hi]
    qd_ref[...] = (q32 * jnp.exp(cum + before[0:1, 0:1])).astype(bf16)
    kd = (k.astype(f32) * jnp.exp(last - cum)).astype(bf16)
    update = lax.dot_general(kd, v, TN, preferred_element_type=f32)
    state[...] = jnp.exp(last) * state[...] + update
    before[...] = before[...] + last

    @pl.when(b == pl.num_programs(0) - 1)
    def _():
        send_ref[0:HEAD_DIM, :] = state[...].astype(bf16)
        put_decay(send_ref, jnp.exp(before[...]))


def put_decay(ref, decay):
    high = decay.astype(bf16)
    low = (decay - high.astype(f32)).astype(bf16)
    ref[HEAD_DIM : HEAD_DIM + 8, :HALF] = jnp.broadcast_to(high, (8, HALF))
    ref[HEAD_DIM : HEAD_DIM + 8, HALF:] = jnp.broadcast_to(low, (8, HALF))


def get_decay(ref):
    tail = ref[HEAD_DIM : HEAD_DIM + 8, :].astype(f32)
    return tail[0:1, 0:1] + tail[0:1, HALF : HALF + 1]


def local_part(base, q, k, v, ld, cos_t, sin_t):
    rows = q.shape[0]
    blocks = rows // BLOCK
    seq = pl.BlockSpec((BLOCK, HEAD_DIM), lambda b: (b, 0))
    table = pl.BlockSpec((BLOCK, HALF), lambda b: (0, 0))
    return pl.pallas_call(
        local_kernel,
        grid=(blocks,),
        out_shape=[
            jax.ShapeDtypeStruct((rows, HEAD_DIM), f32),
            jax.ShapeDtypeStruct((rows, HEAD_DIM), bf16),
            jax.ShapeDtypeStruct((HEAD_DIM + 8, HEAD_DIM), bf16),
        ],
        in_specs=[
            pl.BlockSpec((1, 2, HALF), lambda b: (b, 0, 0)),
            seq,
            seq,
            seq,
            pl.BlockSpec((1, 1, BLOCK), lambda b: (b, 0, 0)),
            table,
            table,
        ],
        out_specs=[seq, seq, pl.BlockSpec((HEAD_DIM + 8, HEAD_DIM), lambda b: (0, 0))],
        scratch_shapes=[
            pltpu.VMEM((HEAD_DIM, HEAD_DIM), f32),
            pltpu.VMEM((8, HALF), f32),
        ],
        compiler_params=grid_params(16),
        cost_estimate=pl.CostEstimate(
            flops=6 * 10**9, bytes_accessed=6 * 2**20, transcendentals=2**20
        ),
        name="local",
    )(base, q, k, v, ld, cos_t, sin_t)


def middle_kernel(x_ref, own_ref, one_ref, two_ref, three_ref, before_ref, send_ref):
    x = x_ref[0]
    refs = (own_ref, one_ref, two_ref, three_ref)
    place = [lax.rem(x - s + 4, 4) for s in range(4)]
    decay = [get_decay(r) for r in refs]
    into = jnp.zeros((HEAD_DIM, HEAD_DIM), f32)
    whole = jnp.zeros((HEAD_DIM, HEAD_DIM), f32)
    through = jnp.ones((1, 1), f32)
    for s in range(4):
        after_all = jnp.ones((1, 1), f32)
        for o in range(4):
            if o != s:
                after_all = after_all * jnp.where(place[o] > place[s], decay[o], 1.0)
        part = refs[s][0:HEAD_DIM, :].astype(f32)
        whole = whole + part * after_all
        if s:
            into = into + jnp.where(s <= x, through, 0.0) * part
            through = through * jnp.where(s <= x, decay[s], 1.0)
    before_ref[0:HEAD_DIM, :] = into
    before_ref[HEAD_DIM : HEAD_DIM + 8, :] = jnp.broadcast_to(through, (8, HEAD_DIM))
    send_ref[0:HEAD_DIM, :] = whole.astype(bf16)
    total = decay[0] * decay[1] * decay[2] * decay[3]
    put_decay(send_ref, jnp.broadcast_to(total, (8, HALF)))


def middle(x, own, one, two, three):
    return pl.pallas_call(
        middle_kernel,
        out_shape=[
            jax.ShapeDtypeStruct((HEAD_DIM + 8, HEAD_DIM), f32),
            jax.ShapeDtypeStruct((HEAD_DIM + 8, HEAD_DIM), bf16),
        ],
        in_specs=[pl.BlockSpec(memory_space=pltpu.SMEM)]
        + [pl.BlockSpec(memory_space=pltpu.VMEM)] * 4,
        out_specs=[pl.BlockSpec(memory_space=pltpu.VMEM)] * 2,
        compiler_params=pltpu.CompilerParams(vmem_limit_bytes=8 * MIB),
        cost_estimate=pl.CostEstimate(
            flops=2 * 10**10, bytes_accessed=10**6, transcendentals=0
        ),
        name="middle",
    )(x, own, one, two, three)


def finish_kernel(
    place_ref,
    before_ref,
    one_ref,
    two_ref,
    three_ref,
    kept_ref,
    qd_ref,
    gate_ref,
    gain_ref,
    out_ref,
    start,
):
    @pl.when(pl.program_id(0) == 0)
    def _():
        into = three_ref[0:HEAD_DIM, :].astype(f32)
        for ref in (two_ref, one_ref):
            into = ref[0:HEAD_DIM, :].astype(f32) + get_decay(ref) * into
        through = before_ref[HEAD_DIM : HEAD_DIM + 1, 0:1]
        start[...] = (before_ref[0:HEAD_DIM, :] + through * into).astype(bf16)

    retained = kept_ref[...] + mm(qd_ref[...], start[...])
    scale = lax.rsqrt(jnp.mean(retained * retained, axis=-1, keepdims=True) + norm_eps)
    gate = gate_ref[...].astype(f32)
    gate = gate / (1.0 + jnp.exp(-gate))
    done = (gate * retained * scale * gain_ref[...]).astype(bf16)
    rows = BLOCK // 2
    for c in range(2):
        other = lax.rem(place_ref[1] + c, 2)
        out_ref[pl.ds(pl.multiple_of(other * rows, rows), rows), :] = done[c * rows : (c + 1) * rows]


def finish(place, before, one, two, three, kept, qd, gate, gain):
    rows = qd.shape[0]
    seq = pl.BlockSpec((BLOCK, HEAD_DIM), lambda b, place: (b, 0))
    whole = pl.BlockSpec((HEAD_DIM + 8, HEAD_DIM), lambda b, place: (0, 0))
    return pl.pallas_call(
        finish_kernel,
        grid_spec=pltpu.PrefetchScalarGridSpec(
            num_scalar_prefetch=1,
            grid=(rows // BLOCK,),
            in_specs=[whole] * 4
            + [seq] * 3
            + [pl.BlockSpec((1, HEAD_DIM), lambda b, place: (0, 0))],
            out_specs=pl.BlockSpec(
                (BLOCK, HEAD_DIM), lambda b, place: (lax.rem(b - place[0] + 4, 4), 0)
            ),
            scratch_shapes=[pltpu.VMEM((HEAD_DIM, HEAD_DIM), bf16)],
        ),
        out_shape=jax.ShapeDtypeStruct((rows, HEAD_DIM), bf16),
        compiler_params=grid_params(12),
        cost_estimate=pl.CostEstimate(
            flops=2 * 10**9, bytes_accessed=5 * 2**20, transcendentals=2**19
        ),
        name="finish",
    )(place, before, one, two, three, kept, qd, gate, gain)


def project_kernel(head_ref, *refs):
    pieces, w_ref, out_ref = refs[:-2], refs[-2], refs[-1]
    total = None
    for s, piece in enumerate(pieces):
        at = pl.multiple_of(head_ref[s] * HEAD_DIM, HEAD_DIM)
        part = mm(piece[...], w_ref[pl.ds(at, HEAD_DIM), :])
        total = part if total is None else total + part
    out_ref[...] = total.astype(bf16)


def project(heads, pieces, w_out):
    whole, width = w_out.shape
    rows = pieces[0].shape[0]
    cols = 256
    return pl.pallas_call(
        project_kernel,
        grid_spec=pltpu.PrefetchScalarGridSpec(
            num_scalar_prefetch=1,
            grid=(width // cols,),
            in_specs=[pl.BlockSpec((rows, HEAD_DIM), lambda n, heads: (0, 0))] * len(pieces)
            + [pl.BlockSpec((whole, cols), lambda n, heads: (0, n))],
            out_specs=pl.BlockSpec((rows, cols), lambda n, heads: (0, n)),
        ),
        out_shape=jax.ShapeDtypeStruct((rows, width), bf16),
        compiler_params=grid_params(12),
        cost_estimate=pl.CostEstimate(
            flops=4 * 10**9, bytes_accessed=10 * 2**20, transcendentals=0
        ),
        name="project",
    )(heads, *pieces, w_out)


def angle_tables():
    inverse = 10000.0 ** (-np.arange(HALF) * 2.0 / HEAD_DIM)
    angle = np.arange(BLOCK)[:, None] * inverse[None, :]
    return np.cos(angle).astype(np.float32), np.sin(angle).astype(np.float32)


def on_device(
    mix_query,
    mix_key,
    mix_value,
    mix_gate,
    log_decay,
    ret_gain,
    w_out,
    moe_in,
    route_ids,
    route_weights,
    moe_gain,
    w_gate,
    w_up,
    w_down,
):
    seq_rows = mix_query.shape[0]
    blocks = seq_rows // BLOCK
    width = moe_in.shape[1]
    ep = ("z", "x")
    tp = ("y", "core")

    ids = route_ids.T
    outgoing = pl.pallas_call(
        pre_kernel,
        out_shape=jax.ShapeDtypeStruct((SLOTS, width), bf16),
        compiler_params=pltpu.CompilerParams(vmem_limit_bytes=8 * MIB),
        cost_estimate=pl.CostEstimate(flops=2 * 10**9, bytes_accessed=10**6, transcendentals=0),
        name="pre",
    )(moe_in, ids, moe_gain.reshape(1, -1))
    own = lax.all_to_all(outgoing, ep, split_axis=0, concat_axis=0, tiled=True)

    cos_t, sin_t = angle_tables()
    inverse = 10000.0 ** (-np.arange(HALF) * 2.0 / HEAD_DIM)
    first = lax.axis_index(ep) * seq_rows + BLOCK * jnp.arange(blocks, dtype=jnp.int32)
    angle = first.astype(f32)[:, None] * jnp.asarray(inverse, f32)[None, :]
    base = jnp.stack([jnp.cos(angle), jnp.sin(angle)], axis=1)
    kept, qd, end = local_part(
        base,
        after(mix_query, outgoing),
        mix_key,
        mix_value,
        log_decay.reshape(blocks, 1, BLOCK),
        jnp.asarray(cos_t),
        jnp.asarray(sin_t),
    )
    by_x = [shift(end, "x", s) for s in (1, 2, 3)]
    own = after(own, end)

    up = shift(own, "y", 1)
    down = shift(own, "y", -1)
    far = shift(own, "y", 2)
    own_c = shift(own, "core", 1, 2)
    x_index = lax.axis_index("x").astype(jnp.int32).reshape(1)
    before, whole = middle(x_index, end, *by_x)
    by_z = [shift(whole, "z", s, wrap=False) for s in (1, 2, 3)]
    up_c = shift(up, "core", 1, 2)
    down_c = shift(down, "core", 1, 2)
    n = own.shape[0]
    weights = (w_gate[0], w_up[0], w_down[0])
    *keep, give1 = ffn([own, up, down], [own_c, up_c, down_c], weights)
    got1 = shift(give1, "core", 1, 2)
    far_c = shift(far, "core", 1, 2)
    near = [
        (k.astype(f32) + got1[i * n : (i + 1) * n].astype(f32)).astype(bf16)
        for i, k in enumerate(keep)
    ]
    back_up = shift(near[1], "y", -1)
    back_down = shift(near[2], "y", 1)
    keep2, give2 = ffn([after(far, near[2])], [far_c], weights)
    got2 = shift(give2, "core", 1, 2)
    back_far = shift((keep2.astype(f32) + got2.astype(f32)).astype(bf16), "y", 2)
    y_index, c_index = lax.axis_index("y"), lax.axis_index("core")
    place = jnp.stack([y_index, c_index]).astype(jnp.int32)
    heads_out = finish(
        place, before, *by_z, kept, qd, mix_gate, ret_gain.reshape(1, -1)
    )
    pieces, sources = [], []
    m = seq_rows // 8
    for dy in range(4):
        for dc in range(2):
            at = (2 * dy + dc) * m
            piece = heads_out[at : at + m]
            if dy or dc:
                pairs = [
                    (2 * y + c, 2 * ((y + dy) % 4) + (c + dc) % 2)
                    for y in range(4)
                    for c in range(2)
                ]
                piece = lax.ppermute(piece, tp, pairs)
            pieces.append(piece)
            sources.append(2 * lax.rem(y_index - dy + 4, 4) + lax.rem(c_index + dc, 2))
    parts = (near[0], back_up, back_down, back_far)
    expert_rows = sum(v.astype(f32) for v in parts).astype(bf16)
    returned = lax.all_to_all(expert_rows, ep, split_axis=0, concat_axis=0, tiled=True)
    mix_out = project(jnp.stack(sources).astype(jnp.int32), pieces, w_out)
    moe_out = pl.pallas_call(
        combine_kernel,
        out_shape=jax.ShapeDtypeStruct(moe_in.shape, bf16),
        compiler_params=pltpu.CompilerParams(vmem_limit_bytes=8 * MIB),
        cost_estimate=pl.CostEstimate(flops=10**9, bytes_accessed=10**6, transcendentals=0),
        name="combine",
    )(returned, ids, route_weights.T)
    return (mix_out, moe_out)


def solution(mesh):
    ep, tp = ("z", "x"), ("y", "core")
    every = ep + tp
    fine = Mesh(mesh.devices.reshape(4, 4, 4, 2), every)
    in_specs = (
        P(ep, tp),
        P(ep, tp),
        P(ep, tp),
        P(ep, tp),
        P(ep, tp),
        P(tp),
        P(),
        P(every, None),
        P(every, None),
        P(every, None),
        P(),
        P(ep, None, tp),
        P(ep, None, tp),
        P(ep, tp, None),
    )
    out_specs = (P(every, None), P(every, None))

    return jax.shard_map(
        on_device, mesh=fine, in_specs=in_specs, out_specs=out_specs, check_vma=False
    )
```

```python
import functools

import jax
import jax.numpy as jnp
import numpy as np
from jax import lax
from jax.experimental import pallas as pl
from jax.experimental.pallas import tpu as pltpu
from jax.sharding import Mesh
from jax.sharding import PartitionSpec as P


HEAD_DIM = 256
HALF = HEAD_DIM // 2
BLOCK = 512
EXPERTS = 16
CAP = 8
SLOTS = EXPERTS * CAP
norm_eps = 1e-06


MIB = 2**20

f32 = jnp.float32
bf16 = jnp.bfloat16

NT = (((1,), (1,)), ((), ()))
TN = (((0,), (0,)), ((), ()))


def mm(a, b):
    return jnp.dot(a, b, preferred_element_type=f32)


def shift(x, axis, by, size=4):
    pairs = [(j, (j + by) % size) for j in range(size)]
    return lax.ppermute(x, axis, pairs)


def vm(x):
    return pltpu.with_memory_space_constraint(x, pltpu.VMEM)


def hb(x):
    return pltpu.with_memory_space_constraint(x, pltpu.HBM)


def grid_params(mib):
    return pltpu.CompilerParams(
        dimension_semantics=("arbitrary",), vmem_limit_bytes=mib * MIB
    )


def after(x, *earlier):
    return lax.optimization_barrier((x, *earlier))[0]


def route_tables(ids_ref):
    tokens = ids_ref.shape[1]
    expert = lax.broadcasted_iota(jnp.int32, (EXPERTS, tokens), 0)
    named = [(ids_ref[k : k + 1, :] == expert).astype(f32) for k in range(2)]
    earlier = (
        lax.broadcasted_iota(jnp.int32, (tokens, tokens), 0)
        < lax.broadcasted_iota(jnp.int32, (tokens, tokens), 1)
    ).astype(f32)
    rank = mm(named[0] + named[1], earlier)
    row = lax.broadcasted_iota(jnp.int32, (SLOTS, EXPERTS), 0)
    col = lax.broadcasted_iota(jnp.int32, (SLOTS, EXPERTS), 1)
    spread = (row // CAP == col).astype(f32)
    slot = (lax.broadcasted_iota(jnp.int32, (SLOTS, tokens), 0) % CAP).astype(f32)
    here = jnp.abs(mm(spread, rank) - slot) < 0.5
    return [jnp.where((mm(spread, n) > 0.5) & here, 1.0, 0.0) for n in named]


def pre_kernel(x_ref, ids_ref, gain_ref, out_ref):
    first, second = route_tables(ids_ref)
    x = x_ref[...].astype(f32)
    scale = lax.rsqrt(jnp.mean(x * x, axis=-1, keepdims=True) + norm_eps)
    normed = (x * scale * gain_ref[...]).astype(bf16)
    out_ref[...] = mm((first + second).astype(bf16), normed).astype(bf16)


def combine_kernel(rows_ref, ids_ref, weights_ref, out_ref):
    tokens = ids_ref.shape[1]
    rows = rows_ref[...]
    diagonal = lax.broadcasted_iota(jnp.int32, (tokens, tokens), 0) == lax.broadcasted_iota(
        jnp.int32, (tokens, tokens), 1
    )
    total = None
    for k, pick in enumerate(route_tables(ids_ref)):
        weight = jnp.sum(
            jnp.where(diagonal, weights_ref[k : k + 1, :], 0.0), axis=1, keepdims=True
        )
        part = lax.dot_general(pick.astype(bf16), rows, TN, preferred_element_type=f32) * weight
        total = part if total is None else total + part
    out_ref[...] = total.astype(bf16)


def ffn_kernel(n_x, *refs):
    xs = refs[:n_x]
    wg, wu, wd = refs[n_x : n_x + 3]
    outs = refs[n_x + 3 : -1]
    hbuf = refs[-1]
    tile = xs[0].shape[0]
    for i in range(n_x):
        x = xs[i][...]
        for at in range(0, hbuf.shape[1], 128):
            w = jnp.concatenate([wg[:, at : at + 128], wu[:, at : at + 128]], axis=1)
            both = mm(x, w)
            gate, up = both[:, :128], both[:, 128:]
            hidden = gate * up / (1.0 + jnp.exp(-gate))
            hbuf[i * tile : (i + 1) * tile, at : at + 128] = hidden.astype(bf16)
    keep = len(outs) - 1
    for i in range(n_x):
        out = mm(hbuf[i * tile : (i + 1) * tile, :], wd[...]).astype(bf16)
        if i < keep:
            outs[i][...] = out
        else:
            at = (i - keep) * tile
            outs[keep][at : at + tile, :] = out


def ffn(keep, give, weights):
    n_x = len(keep) + len(give)
    tile, width = keep[0].shape
    ff = weights[0].shape[1]
    rows = n_x * tile
    in_vmem = pl.BlockSpec(memory_space=pltpu.VMEM)
    return pl.pallas_call(
        functools.partial(ffn_kernel, n_x),
        out_shape=[pltpu.VMEM((tile, width), bf16)] * len(keep)
        + [pltpu.VMEM((len(give) * tile, width), bf16)],
        in_specs=[in_vmem] * (n_x + 3),
        out_specs=[in_vmem] * (len(keep) + 1),
        scratch_shapes=[pltpu.VMEM((rows, ff), bf16)],
        compiler_params=pltpu.CompilerParams(vmem_limit_bytes=30 * MIB),
        cost_estimate=pl.CostEstimate(
            flops=6 * rows * width * ff,
            bytes_accessed=2 * (3 * width * ff + 2 * rows * width),
            transcendentals=rows * ff,
        ),
    )(*[vm(x) for x in (*keep, *give)], *weights)


def local_kernel(
    base_ref,
    q_ref,
    k_ref,
    v_ref,
    ld_ref,
    cos_ref,
    sin_ref,
    kept_ref,
    qd_ref,
    send_ref,
    state,
    before,
):
    b = pl.program_id(0)

    @pl.when(b == 0)
    def _():
        state[...] = jnp.zeros_like(state)
        before[...] = jnp.zeros_like(before)

    cos_base = base_ref[0, 0:1, :]
    sin_base = base_ref[0, 1:2, :]
    cos_t, sin_t = cos_ref[...], sin_ref[...]
    cosine = cos_t * cos_base - sin_t * sin_base
    sine = sin_t * cos_base + cos_t * sin_base

    def rotated(ref):
        front = ref[:, :HALF].astype(f32)
        back = ref[:, HALF:].astype(f32)
        return jnp.concatenate([front * cosine - back * sine, back * cosine + front * sine], axis=1)

    q = rotated(q_ref).astype(bf16)
    k = (rotated(k_ref) * HEAD_DIM ** (-0.5)).astype(bf16)
    v = v_ref[...]
    row = lax.broadcasted_iota(jnp.int32, (BLOCK, BLOCK), 0)
    col = lax.broadcasted_iota(jnp.int32, (BLOCK, BLOCK), 1)
    ld = ld_ref[0]
    cum = jnp.sum(jnp.where(row >= col, ld, 0.0), axis=1, keepdims=True)
    cum_row = jnp.sum(jnp.where(row == col, cum, 0.0), axis=0, keepdims=True)
    last = cum[BLOCK - 1 : BLOCK, :]

    q32 = q.astype(f32)
    begin = state[...].astype(bf16)
    carried = mm((q32 * jnp.exp(cum)).astype(bf16), begin)
    half = BLOCK // 2
    for r in range(2):
        lo, hi = r * half, (r + 1) * half
        scores = lax.dot_general(q[lo:hi], k[:hi], NT, preferred_element_type=f32)
        gap = cum[lo:hi] - cum_row[:, :hi]
        seen = (
            lax.broadcasted_iota(jnp.int32, (half, hi), 0) + lo
            >= lax.broadcasted_iota(jnp.int32, (half, hi), 1)
        )
        weights = jnp.where(seen, scores * jnp.exp(jnp.where(seen, gap, 0.0)), 0.0).astype(bf16)
        kept_ref[lo:hi, :] = (mm(weights, v[:hi]) + carried[lo:hi]).astype(bf16)
    qd_ref[...] = (q32 * jnp.exp(cum + before[0:1, 0:1])).astype(bf16)
    kd = (k.astype(f32) * jnp.exp(last - cum)).astype(bf16)
    update = lax.dot_general(kd, v, TN, preferred_element_type=f32)
    state[...] = jnp.exp(last) * state[...] + update
    before[...] = before[...] + last

    @pl.when(b == pl.num_programs(0) - 1)
    def _():
        send_ref[0:HEAD_DIM, :] = state[...].astype(bf16)
        put_decay(send_ref, jnp.exp(before[...]))


def put_decay(ref, decay):
    high = decay.astype(bf16)
    low = (decay - high.astype(f32)).astype(bf16)
    ref[HEAD_DIM : HEAD_DIM + 8, :HALF] = jnp.broadcast_to(high, (8, HALF))
    ref[HEAD_DIM : HEAD_DIM + 8, HALF:] = jnp.broadcast_to(low, (8, HALF))


def get_decay(ref):
    tail = ref[HEAD_DIM : HEAD_DIM + 8, :].astype(f32)
    return tail[0:1, 0:1] + tail[0:1, HALF : HALF + 1]


def local_part(base, q, k, v, ld, cos_t, sin_t):
    rows = q.shape[0]
    blocks = rows // BLOCK
    seq = pl.BlockSpec((BLOCK, HEAD_DIM), lambda b: (b, 0))
    table = pl.BlockSpec((BLOCK, HALF), lambda b: (0, 0))
    return pl.pallas_call(
        local_kernel,
        grid=(blocks,),
        out_shape=[
            pltpu.HBM((rows, HEAD_DIM), bf16),
            pltpu.HBM((rows, HEAD_DIM), bf16),
            jax.ShapeDtypeStruct((HEAD_DIM + 8, HEAD_DIM), bf16),
        ],
        in_specs=[
            pl.BlockSpec((1, 2, HALF), lambda b: (b, 0, 0)),
            seq,
            seq,
            seq,
            pl.BlockSpec((1, 1, BLOCK), lambda b: (b, 0, 0)),
            table,
            table,
        ],
        out_specs=[seq, seq, pl.BlockSpec((HEAD_DIM + 8, HEAD_DIM), lambda b: (0, 0))],
        scratch_shapes=[
            pltpu.VMEM((HEAD_DIM, HEAD_DIM), f32),
            pltpu.VMEM((8, HALF), f32),
        ],
        compiler_params=grid_params(16),
        cost_estimate=pl.CostEstimate(
            flops=6 * 10**9, bytes_accessed=6 * 2**20, transcendentals=2**20
        ),
        name="local",
    )(base, q, k, hb(v), ld, cos_t, sin_t)


def middle_kernel(x_ref, own_ref, one_ref, two_ref, three_ref, before_ref, send_ref):
    x = x_ref[0]
    refs = (own_ref, one_ref, two_ref, three_ref)
    place = [lax.rem(x - s + 4, 4) for s in range(4)]
    decay = [get_decay(r) for r in refs]
    into = jnp.zeros((HEAD_DIM, HEAD_DIM), f32)
    whole = jnp.zeros((HEAD_DIM, HEAD_DIM), f32)
    through = jnp.ones((1, 1), f32)
    for s in range(4):
        after_all = jnp.ones((1, 1), f32)
        for o in range(4):
            if o != s:
                after_all = after_all * jnp.where(place[o] > place[s], decay[o], 1.0)
        part = refs[s][0:HEAD_DIM, :].astype(f32)
        whole = whole + part * after_all
        if s:
            into = into + jnp.where(s <= x, through, 0.0) * part
            through = through * jnp.where(s <= x, decay[s], 1.0)
    before_ref[0:HEAD_DIM, :] = into
    before_ref[HEAD_DIM : HEAD_DIM + 8, :] = jnp.broadcast_to(through, (8, HEAD_DIM))
    send_ref[0:HEAD_DIM, :] = whole.astype(bf16)
    total = decay[0] * decay[1] * decay[2] * decay[3]
    put_decay(send_ref, jnp.broadcast_to(total, (8, HALF)))


def middle(x, own, one, two, three):
    return pl.pallas_call(
        middle_kernel,
        out_shape=[
            jax.ShapeDtypeStruct((HEAD_DIM + 8, HEAD_DIM), f32),
            jax.ShapeDtypeStruct((HEAD_DIM + 8, HEAD_DIM), bf16),
        ],
        in_specs=[pl.BlockSpec(memory_space=pltpu.SMEM)]
        + [pl.BlockSpec(memory_space=pltpu.VMEM)] * 4,
        out_specs=[pl.BlockSpec(memory_space=pltpu.VMEM)] * 2,
        compiler_params=pltpu.CompilerParams(vmem_limit_bytes=8 * MIB),
        cost_estimate=pl.CostEstimate(
            flops=2 * 10**10, bytes_accessed=10**6, transcendentals=0
        ),
        name="middle",
    )(x, own, one, two, three)


def finish_kernel(
    place_ref,
    before_ref,
    one_ref,
    two_ref,
    three_ref,
    kept_ref,
    qd_ref,
    gate_ref,
    gain_ref,
    out_ref,
    start,
):
    @pl.when(pl.program_id(0) == 0)
    def _():
        into = jnp.zeros((HEAD_DIM, HEAD_DIM), f32)
        for far, ref in ((3, three_ref), (2, two_ref), (1, one_ref)):
            longer = ref[0:HEAD_DIM, :].astype(f32) + get_decay(ref) * into
            into = jnp.where(far <= place_ref[0], longer, into)
        through = before_ref[HEAD_DIM : HEAD_DIM + 1, 0:1]
        start[...] = (before_ref[0:HEAD_DIM, :] + through * into).astype(bf16)

    retained = kept_ref[...].astype(f32) + mm(qd_ref[...], start[...])
    scale = lax.rsqrt(jnp.mean(retained * retained, axis=-1, keepdims=True) + norm_eps)
    gate = gate_ref[...].astype(f32)
    gate = gate / (1.0 + jnp.exp(-gate))
    done = (gate * retained * scale * gain_ref[...]).astype(bf16)
    rows = BLOCK // 2
    for c in range(2):
        other = lax.rem(place_ref[2] + c, 2)
        out_ref[pl.ds(pl.multiple_of(other * rows, rows), rows), :] = done[c * rows : (c + 1) * rows]


def finish(place, before, one, two, three, kept, qd, gate, gain):
    rows = qd.shape[0]
    seq = pl.BlockSpec((BLOCK, HEAD_DIM), lambda b, place: (b, 0))
    whole = pl.BlockSpec((HEAD_DIM + 8, HEAD_DIM), lambda b, place: (0, 0))
    return pl.pallas_call(
        finish_kernel,
        grid_spec=pltpu.PrefetchScalarGridSpec(
            num_scalar_prefetch=1,
            grid=(rows // BLOCK,),
            in_specs=[whole] * 4
            + [seq] * 3
            + [pl.BlockSpec((1, HEAD_DIM), lambda b, place: (0, 0))],
            out_specs=pl.BlockSpec(
                (BLOCK, HEAD_DIM), lambda b, place: (lax.rem(b - place[1] + 4, 4), 0)
            ),
            scratch_shapes=[pltpu.VMEM((HEAD_DIM, HEAD_DIM), bf16)],
        ),
        out_shape=jax.ShapeDtypeStruct((rows, HEAD_DIM), bf16),
        compiler_params=grid_params(12),
        cost_estimate=pl.CostEstimate(
            flops=2 * 10**9, bytes_accessed=5 * 2**20, transcendentals=2**19
        ),
        name="finish",
    )(place, before, one, two, three, hb(kept), hb(qd), hb(gate), hb(gain))


def project_kernel(head_ref, *refs):
    pieces, w_ref, out_ref = refs[:-2], refs[-2], refs[-1]
    total = None
    for s, piece in enumerate(pieces):
        at = pl.multiple_of(head_ref[s] * HEAD_DIM, HEAD_DIM)
        part = mm(piece[...], w_ref[pl.ds(at, HEAD_DIM), :])
        total = part if total is None else total + part
    out_ref[...] = total.astype(bf16)


def project(heads, pieces, w_out):
    whole, width = w_out.shape
    rows = pieces[0].shape[0]
    cols = 512
    return pl.pallas_call(
        project_kernel,
        grid_spec=pltpu.PrefetchScalarGridSpec(
            num_scalar_prefetch=1,
            grid=(width // cols,),
            in_specs=[pl.BlockSpec((rows, HEAD_DIM), lambda n, heads: (0, 0))] * len(pieces)
            + [pl.BlockSpec((whole, cols), lambda n, heads: (0, n))],
            out_specs=pl.BlockSpec((rows, cols), lambda n, heads: (0, n)),
        ),
        out_shape=jax.ShapeDtypeStruct((rows, width), bf16),
        compiler_params=grid_params(12),
        cost_estimate=pl.CostEstimate(
            flops=4 * 10**9, bytes_accessed=10 * 2**20, transcendentals=0
        ),
        name="project",
    )(heads, *pieces, w_out)


def angle_tables():
    inverse = 10000.0 ** (-np.arange(HALF) * 2.0 / HEAD_DIM)
    angle = np.arange(BLOCK)[:, None] * inverse[None, :]
    return np.cos(angle).astype(np.float32), np.sin(angle).astype(np.float32)


def on_device(
    mix_query,
    mix_key,
    mix_value,
    mix_gate,
    log_decay,
    ret_gain,
    w_out,
    moe_in,
    route_ids,
    route_weights,
    moe_gain,
    w_gate,
    w_up,
    w_down,
):
    seq_rows = mix_query.shape[0]
    blocks = seq_rows // BLOCK
    width = moe_in.shape[1]
    ep = ("z", "x")
    tp = ("y", "core")

    ids = route_ids.T
    outgoing = pl.pallas_call(
        pre_kernel,
        out_shape=jax.ShapeDtypeStruct((SLOTS, width), bf16),
        compiler_params=pltpu.CompilerParams(vmem_limit_bytes=8 * MIB),
        cost_estimate=pl.CostEstimate(flops=2 * 10**9, bytes_accessed=10**6, transcendentals=0),
        name="pre",
    )(hb(moe_in), hb(ids), hb(moe_gain.reshape(1, -1)))
    own = lax.all_to_all(outgoing, ep, split_axis=0, concat_axis=0, tiled=True)

    cos_t, sin_t = angle_tables()
    inverse = 10000.0 ** (-np.arange(HALF) * 2.0 / HEAD_DIM)
    first = lax.axis_index(ep) * seq_rows + BLOCK * jnp.arange(blocks, dtype=jnp.int32)
    angle = first.astype(f32)[:, None] * jnp.asarray(inverse, f32)[None, :]
    base = jnp.stack([jnp.cos(angle), jnp.sin(angle)], axis=1)
    kept, qd, end = local_part(
        base,
        after(mix_query, outgoing),
        mix_key,
        mix_value,
        log_decay.reshape(blocks, 1, BLOCK),
        jnp.asarray(cos_t),
        jnp.asarray(sin_t),
    )
    by_x = [shift(end, "x", s) for s in (1, 2, 3)]
    own = after(own, end)

    up = shift(own, "y", 1)
    down = shift(own, "y", -1)
    far = shift(own, "y", 2)
    own_c = shift(own, "core", 1, 2)
    x_index = lax.axis_index("x").astype(jnp.int32).reshape(1)
    before, whole = middle(x_index, end, *by_x)
    by_z = [shift(whole, "z", s) for s in (1, 2, 3)]
    up_c = shift(up, "core", 1, 2)
    down_c = shift(down, "core", 1, 2)
    n = own.shape[0]
    weights = (w_gate[0], w_up[0], w_down[0])
    *keep, give1 = ffn([own, up, down], [own_c, up_c, down_c], weights)
    got1 = shift(give1, "core", 1, 2)
    far_c = shift(far, "core", 1, 2)
    near = [
        (k.astype(f32) + got1[i * n : (i + 1) * n].astype(f32)).astype(bf16)
        for i, k in enumerate(keep)
    ]
    near = lax.optimization_barrier(near)
    back_up = shift(near[1], "y", -1)
    back_down = shift(near[2], "y", 1)
    keep2, give2 = ffn([after(far, near[2])], [far_c], weights)
    got2 = shift(give2, "core", 1, 2)
    back_far = shift((keep2.astype(f32) + got2.astype(f32)).astype(bf16), "y", 2)
    y_at, c_at = lax.axis_index("y"), lax.axis_index("core")
    place = jnp.stack([lax.axis_index("z"), y_at, c_at]).astype(jnp.int32)
    heads_out = finish(
        place, before, *by_z, kept, qd, mix_gate, ret_gain.reshape(1, -1)
    )
    pieces, sources = [], []
    m = seq_rows // 8
    for dy in range(4):
        for dc in range(2):
            at = (2 * dy + dc) * m
            piece = heads_out[at : at + m]
            if dy or dc:
                pairs = [
                    (2 * y + c, 2 * ((y + dy) % 4) + (c + dc) % 2)
                    for y in range(4)
                    for c in range(2)
                ]
                piece = lax.ppermute(piece, tp, pairs)
            pieces.append(piece)
            sources.append(2 * lax.rem(y_at - dy + 4, 4) + lax.rem(c_at + dc, 2))
    parts = (near[0], back_up, back_down, back_far)
    expert_rows = sum(v.astype(f32) for v in parts).astype(bf16)
    returned = lax.all_to_all(expert_rows, ep, split_axis=0, concat_axis=0, tiled=True)
    mix_out = project(jnp.stack(sources).astype(jnp.int32), pieces, w_out)
    moe_out = pl.pallas_call(
        combine_kernel,
        out_shape=jax.ShapeDtypeStruct(moe_in.shape, bf16),
        compiler_params=pltpu.CompilerParams(vmem_limit_bytes=8 * MIB),
        cost_estimate=pl.CostEstimate(flops=10**9, bytes_accessed=10**6, transcendentals=0),
        name="combine",
    )(returned, ids, route_weights.T)
    return (mix_out, moe_out)


def solution(mesh):
    ep, tp = ("z", "x"), ("y", "core")
    every = ep + tp
    fine = Mesh(mesh.devices.reshape(4, 4, 4, 2), every)
    in_specs = (
        P(ep, tp),
        P(ep, tp),
        P(ep, tp),
        P(ep, tp),
        P(ep, tp),
        P(tp),
        P(),
        P(every, None),
        P(every, None),
        P(every, None),
        P(),
        P(ep, None, tp),
        P(ep, None, tp),
        P(ep, tp, None),
    )
    out_specs = (P(every, None), P(every, None))

    return jax.shard_map(
        on_device, mesh=fine, in_specs=in_specs, out_specs=out_specs, check_vma=False
    )
```

```python
import functools

import jax
import jax.numpy as jnp
import numpy as np
from jax import lax
from jax.experimental import pallas as pl
from jax.experimental.pallas import tpu as pltpu
from jax.sharding import Mesh
from jax.sharding import PartitionSpec as P


HEAD_DIM = 256
HALF = HEAD_DIM // 2
BLOCK = 512
EXPERTS = 16
CAP = 8
SLOTS = EXPERTS * CAP
norm_eps = 1e-06


MIB = 2**20

f32 = jnp.float32
bf16 = jnp.bfloat16

NT = (((1,), (1,)), ((), ()))
TN = (((0,), (0,)), ((), ()))


def mm(a, b):
    return jnp.dot(a, b, preferred_element_type=f32)


def shift(x, axis, by, size=4):
    pairs = [(j, (j + by) % size) for j in range(size)]
    return lax.ppermute(x, axis, pairs)


def vm(x):
    return pltpu.with_memory_space_constraint(x, pltpu.VMEM)


def hb(x):
    return pltpu.with_memory_space_constraint(x, pltpu.HBM)


def grid_params(mib):
    return pltpu.CompilerParams(
        dimension_semantics=("arbitrary",), vmem_limit_bytes=mib * MIB
    )


def after(x, *earlier):
    return lax.optimization_barrier((x, *earlier))[0]


def route_tables(ids_ref):
    tokens = ids_ref.shape[1]
    expert = lax.broadcasted_iota(jnp.int32, (EXPERTS, tokens), 0)
    named = [(ids_ref[k : k + 1, :] == expert).astype(f32) for k in range(2)]
    earlier = (
        lax.broadcasted_iota(jnp.int32, (tokens, tokens), 0)
        < lax.broadcasted_iota(jnp.int32, (tokens, tokens), 1)
    ).astype(f32)
    rank = mm(named[0] + named[1], earlier)
    row = lax.broadcasted_iota(jnp.int32, (SLOTS, EXPERTS), 0)
    col = lax.broadcasted_iota(jnp.int32, (SLOTS, EXPERTS), 1)
    spread = (row // CAP == col).astype(f32)
    slot = (lax.broadcasted_iota(jnp.int32, (SLOTS, tokens), 0) % CAP).astype(f32)
    here = jnp.abs(mm(spread, rank) - slot) < 0.5
    return [jnp.where((mm(spread, n) > 0.5) & here, 1.0, 0.0) for n in named]


def pre_kernel(x_ref, ids_ref, gain_ref, out_ref):
    first, second = route_tables(ids_ref)
    x = x_ref[...].astype(f32)
    scale = lax.rsqrt(jnp.mean(x * x, axis=-1, keepdims=True) + norm_eps)
    normed = (x * scale * gain_ref[...]).astype(bf16)
    out_ref[...] = mm((first + second).astype(bf16), normed).astype(bf16)


def combine_kernel(rows_ref, ids_ref, weights_ref, out_ref):
    tokens = ids_ref.shape[1]
    rows = rows_ref[...]
    diagonal = lax.broadcasted_iota(jnp.int32, (tokens, tokens), 0) == lax.broadcasted_iota(
        jnp.int32, (tokens, tokens), 1
    )
    total = None
    for k, pick in enumerate(route_tables(ids_ref)):
        weight = jnp.sum(
            jnp.where(diagonal, weights_ref[k : k + 1, :], 0.0), axis=1, keepdims=True
        )
        part = lax.dot_general(pick.astype(bf16), rows, TN, preferred_element_type=f32) * weight
        total = part if total is None else total + part
    out_ref[...] = total.astype(bf16)


def ffn_kernel(n_x, *refs):
    xs = refs[:n_x]
    wg, wu, wd = refs[n_x : n_x + 3]
    outs = refs[n_x + 3 : -1]
    hbuf = refs[-1]
    tile = xs[0].shape[0]
    for i in range(n_x):
        x = xs[i][...]
        for at in range(0, hbuf.shape[1], 128):
            w = jnp.concatenate([wg[:, at : at + 128], wu[:, at : at + 128]], axis=1)
            both = mm(x, w)
            gate, up = both[:, :128], both[:, 128:]
            hidden = gate * up / (1.0 + jnp.exp(-gate))
            hbuf[i * tile : (i + 1) * tile, at : at + 128] = hidden.astype(bf16)
    keep = len(outs) - 1
    for i in range(n_x):
        out = mm(hbuf[i * tile : (i + 1) * tile, :], wd[...]).astype(bf16)
        if i < keep:
            outs[i][...] = out
        else:
            at = (i - keep) * tile
            outs[keep][at : at + tile, :] = out


def ffn(keep, give, weights):
    n_x = len(keep) + len(give)
    tile, width = keep[0].shape
    ff = weights[0].shape[1]
    rows = n_x * tile
    in_vmem = pl.BlockSpec(memory_space=pltpu.VMEM)
    return pl.pallas_call(
        functools.partial(ffn_kernel, n_x),
        out_shape=[pltpu.VMEM((tile, width), bf16)] * len(keep)
        + [pltpu.VMEM((len(give) * tile, width), bf16)],
        in_specs=[in_vmem] * (n_x + 3),
        out_specs=[in_vmem] * (len(keep) + 1),
        scratch_shapes=[pltpu.VMEM((rows, ff), bf16)],
        compiler_params=pltpu.CompilerParams(vmem_limit_bytes=30 * MIB),
        cost_estimate=pl.CostEstimate(
            flops=6 * rows * width * ff,
            bytes_accessed=2 * (3 * width * ff + 2 * rows * width),
            transcendentals=rows * ff,
        ),
    )(*[vm(x) for x in (*keep, *give)], *weights)


def sum_kernel(plan, n_in, *refs):
    outs = refs[n_in:]
    for out, terms in zip(outs, plan, strict=True):
        rows = out.shape[0]
        total = None
        for i, at in terms:
            term = refs[i][at : at + rows, :].astype(f32)
            total = term if total is None else total + term
        out[...] = total.astype(bf16)


def sums(arrays, plan):
    rows, width = arrays[0].shape
    in_vmem = pl.BlockSpec(memory_space=pltpu.VMEM)
    return pl.pallas_call(
        functools.partial(sum_kernel, plan, len(arrays)),
        out_shape=[pltpu.VMEM((rows, width), bf16)] * len(plan),
        in_specs=[in_vmem] * len(arrays),
        out_specs=[in_vmem] * len(plan),
        compiler_params=pltpu.CompilerParams(vmem_limit_bytes=8 * MIB),
        cost_estimate=pl.CostEstimate(
            flops=10**9, bytes_accessed=2 * 2**20, transcendentals=0
        ),
    )(*[vm(v) for v in arrays])


def local_kernel(
    base_ref,
    q_ref,
    k_ref,
    v_ref,
    ld_ref,
    cos_ref,
    sin_ref,
    kept_ref,
    qd_ref,
    send_ref,
    state,
    before,
):
    b = pl.program_id(0)

    @pl.when(b == 0)
    def _():
        state[...] = jnp.zeros_like(state)
        before[...] = jnp.zeros_like(before)

    cos_base = base_ref[0, 0:1, :]
    sin_base = base_ref[0, 1:2, :]
    cos_t, sin_t = cos_ref[...], sin_ref[...]
    cosine = cos_t * cos_base - sin_t * sin_base
    sine = sin_t * cos_base + cos_t * sin_base

    def rotated(ref):
        front = ref[:, :HALF].astype(f32)
        back = ref[:, HALF:].astype(f32)
        return jnp.concatenate([front * cosine - back * sine, back * cosine + front * sine], axis=1)

    q = rotated(q_ref).astype(bf16)
    k = (rotated(k_ref) * HEAD_DIM ** (-0.5)).astype(bf16)
    v = v_ref[...]
    row = lax.broadcasted_iota(jnp.int32, (BLOCK, BLOCK), 0)
    col = lax.broadcasted_iota(jnp.int32, (BLOCK, BLOCK), 1)
    ld = ld_ref[0]
    cum = jnp.sum(jnp.where(row >= col, ld, 0.0), axis=1, keepdims=True)
    cum_row = jnp.sum(jnp.where(row == col, cum, 0.0), axis=0, keepdims=True)
    last = cum[BLOCK - 1 : BLOCK, :]

    q32 = q.astype(f32)
    begin = state[...].astype(bf16)
    carried = mm((q32 * jnp.exp(cum)).astype(bf16), begin)
    half = BLOCK // 2
    for r in range(2):
        lo, hi = r * half, (r + 1) * half
        scores = lax.dot_general(q[lo:hi], k[:hi], NT, preferred_element_type=f32)
        gap = cum[lo:hi] - cum_row[:, :hi]
        seen = (
            lax.broadcasted_iota(jnp.int32, (half, hi), 0) + lo
            >= lax.broadcasted_iota(jnp.int32, (half, hi), 1)
        )
        weights = jnp.where(seen, scores * jnp.exp(jnp.where(seen, gap, 0.0)), 0.0).astype(bf16)
        kept_ref[lo:hi, :] = (mm(weights, v[:hi]) + carried[lo:hi]).astype(bf16)
    qd_ref[...] = (q32 * jnp.exp(cum + before[0:1, 0:1])).astype(bf16)
    kd = (k.astype(f32) * jnp.exp(last - cum)).astype(bf16)
    update = lax.dot_general(kd, v, TN, preferred_element_type=f32)
    state[...] = jnp.exp(last) * state[...] + update
    before[...] = before[...] + last

    @pl.when(b == pl.num_programs(0) - 1)
    def _():
        send_ref[0:HEAD_DIM, :] = state[...].astype(bf16)
        put_decay(send_ref, jnp.exp(before[...]))


def put_decay(ref, decay):
    high = decay.astype(bf16)
    low = (decay - high.astype(f32)).astype(bf16)
    ref[HEAD_DIM : HEAD_DIM + 8, :HALF] = jnp.broadcast_to(high, (8, HALF))
    ref[HEAD_DIM : HEAD_DIM + 8, HALF:] = jnp.broadcast_to(low, (8, HALF))


def get_decay(ref):
    tail = ref[HEAD_DIM : HEAD_DIM + 8, :].astype(f32)
    return tail[0:1, 0:1] + tail[0:1, HALF : HALF + 1]


def local_part(base, q, k, v, ld, cos_t, sin_t):
    rows = q.shape[0]
    blocks = rows // BLOCK
    seq = pl.BlockSpec((BLOCK, HEAD_DIM), lambda b: (b, 0))
    table = pl.BlockSpec((BLOCK, HALF), lambda b: (0, 0))
    return pl.pallas_call(
        local_kernel,
        grid=(blocks,),
        out_shape=[
            pltpu.HBM((rows, HEAD_DIM), bf16),
            pltpu.HBM((rows, HEAD_DIM), bf16),
            jax.ShapeDtypeStruct((HEAD_DIM + 8, HEAD_DIM), bf16),
        ],
        in_specs=[
            pl.BlockSpec((1, 2, HALF), lambda b: (b, 0, 0)),
            seq,
            seq,
            seq,
            pl.BlockSpec((1, 1, BLOCK), lambda b: (b, 0, 0)),
            table,
            table,
        ],
        out_specs=[seq, seq, pl.BlockSpec((HEAD_DIM + 8, HEAD_DIM), lambda b: (0, 0))],
        scratch_shapes=[
            pltpu.VMEM((HEAD_DIM, HEAD_DIM), f32),
            pltpu.VMEM((8, HALF), f32),
        ],
        compiler_params=grid_params(16),
        cost_estimate=pl.CostEstimate(
            flops=6 * 10**9, bytes_accessed=6 * 2**20, transcendentals=2**20
        ),
        name="local",
    )(base, q, k, hb(v), ld, cos_t, sin_t)


def middle_kernel(x_ref, own_ref, one_ref, two_ref, three_ref, before_ref, send_ref):
    x = x_ref[0]
    refs = (own_ref, one_ref, two_ref, three_ref)
    place = [lax.rem(x - s + 4, 4) for s in range(4)]
    decay = [get_decay(r) for r in refs]
    into = jnp.zeros((HEAD_DIM, HEAD_DIM), f32)
    whole = jnp.zeros((HEAD_DIM, HEAD_DIM), f32)
    through = jnp.ones((1, 1), f32)
    for s in range(4):
        after_all = jnp.ones((1, 1), f32)
        for o in range(4):
            if o != s:
                after_all = after_all * jnp.where(place[o] > place[s], decay[o], 1.0)
        part = refs[s][0:HEAD_DIM, :].astype(f32)
        whole = whole + part * after_all
        if s:
            into = into + jnp.where(s <= x, through, 0.0) * part
            through = through * jnp.where(s <= x, decay[s], 1.0)
    before_ref[0:HEAD_DIM, :] = into
    before_ref[HEAD_DIM : HEAD_DIM + 8, :] = jnp.broadcast_to(through, (8, HEAD_DIM))
    send_ref[0:HEAD_DIM, :] = whole.astype(bf16)
    total = decay[0] * decay[1] * decay[2] * decay[3]
    put_decay(send_ref, jnp.broadcast_to(total, (8, HALF)))


def middle(x, own, one, two, three):
    return pl.pallas_call(
        middle_kernel,
        out_shape=[
            pltpu.HBM((HEAD_DIM + 8, HEAD_DIM), f32),
            jax.ShapeDtypeStruct((HEAD_DIM + 8, HEAD_DIM), bf16),
        ],
        in_specs=[pl.BlockSpec(memory_space=pltpu.SMEM)]
        + [pl.BlockSpec(memory_space=pltpu.VMEM)] * 4,
        out_specs=[pl.BlockSpec(memory_space=pltpu.VMEM)] * 2,
        compiler_params=pltpu.CompilerParams(vmem_limit_bytes=8 * MIB),
        cost_estimate=pl.CostEstimate(
            flops=2 * 10**10, bytes_accessed=10**6, transcendentals=0
        ),
        name="middle",
    )(x, own, one, two, three)


def finish_kernel(
    place_ref,
    before_ref,
    one_ref,
    two_ref,
    three_ref,
    kept_ref,
    qd_ref,
    gate_ref,
    gain_ref,
    out_ref,
    start,
):
    @pl.when(pl.program_id(0) == 0)
    def _():
        into = jnp.zeros((HEAD_DIM, HEAD_DIM), f32)
        for far, ref in ((3, three_ref), (2, two_ref), (1, one_ref)):
            longer = ref[0:HEAD_DIM, :].astype(f32) + get_decay(ref) * into
            into = jnp.where(far <= place_ref[0], longer, into)
        through = before_ref[HEAD_DIM : HEAD_DIM + 1, 0:1]
        start[...] = (before_ref[0:HEAD_DIM, :] + through * into).astype(bf16)

    retained = kept_ref[...].astype(f32) + mm(qd_ref[...], start[...])
    scale = lax.rsqrt(jnp.mean(retained * retained, axis=-1, keepdims=True) + norm_eps)
    gate = gate_ref[...].astype(f32)
    gate = gate / (1.0 + jnp.exp(-gate))
    done = (gate * retained * scale * gain_ref[...]).astype(bf16)
    rows = BLOCK // 2
    for c in range(2):
        other = lax.rem(place_ref[2] + c, 2)
        out_ref[pl.ds(pl.multiple_of(other * rows, rows), rows), :] = done[c * rows : (c + 1) * rows]


def finish(place, before, one, two, three, kept, qd, gate, gain):
    rows = qd.shape[0]
    seq = pl.BlockSpec((BLOCK, HEAD_DIM), lambda b, place: (b, 0))
    whole = pl.BlockSpec((HEAD_DIM + 8, HEAD_DIM), lambda b, place: (0, 0))
    return pl.pallas_call(
        finish_kernel,
        grid_spec=pltpu.PrefetchScalarGridSpec(
            num_scalar_prefetch=1,
            grid=(rows // BLOCK,),
            in_specs=[whole] * 4
            + [seq] * 3
            + [pl.BlockSpec((1, HEAD_DIM), lambda b, place: (0, 0))],
            out_specs=pl.BlockSpec(
                (BLOCK, HEAD_DIM), lambda b, place: (lax.rem(b - place[1] + 4, 4), 0)
            ),
            scratch_shapes=[pltpu.VMEM((HEAD_DIM, HEAD_DIM), bf16)],
        ),
        out_shape=jax.ShapeDtypeStruct((rows, HEAD_DIM), bf16),
        compiler_params=grid_params(12),
        cost_estimate=pl.CostEstimate(
            flops=2 * 10**9, bytes_accessed=5 * 2**20, transcendentals=2**19
        ),
        name="finish",
    )(place, hb(before), one, two, three, hb(kept), hb(qd), hb(gate), hb(gain))


def project_kernel(head_ref, *refs):
    pieces, w_ref, out_ref, buf, sems = refs[:-4], *refs[-4:]
    cols = out_ref.shape[1] // sems.shape[0]
    copies = []
    for n in range(sems.shape[0]):
        at = pl.ds(n * cols, cols)
        c = pltpu.make_async_copy(w_ref.at[:, at], buf.at[:, at], sems.at[n])
        c.start()
        copies.append(c)
    for n, c in enumerate(copies):
        c.wait()
        total = None
        for s, piece in enumerate(pieces):
            at = pl.multiple_of(head_ref[s] * HEAD_DIM, HEAD_DIM)
            part = mm(piece[...], buf[pl.ds(at, HEAD_DIM), n * cols : (n + 1) * cols])
            total = part if total is None else total + part
        out_ref[:, n * cols : (n + 1) * cols] = total.astype(bf16)


def project(heads, pieces, w_out):
    whole, width = w_out.shape
    rows = pieces[0].shape[0]
    in_vmem = pl.BlockSpec(memory_space=pltpu.VMEM)
    return pl.pallas_call(
        project_kernel,
        out_shape=jax.ShapeDtypeStruct((rows, width), bf16),
        in_specs=[pl.BlockSpec(memory_space=pltpu.SMEM)]
        + [in_vmem] * len(pieces)
        + [pl.BlockSpec(memory_space=pl.ANY)],
        out_specs=in_vmem,
        scratch_shapes=[pltpu.VMEM((whole, width), bf16), pltpu.SemaphoreType.DMA((4,))],
        compiler_params=pltpu.CompilerParams(vmem_limit_bytes=16 * MIB),
        cost_estimate=pl.CostEstimate(
            flops=4 * 10**9, bytes_accessed=10 * 2**20, transcendentals=0
        ),
        name="project",
    )(heads, *[vm(v) for v in pieces], hb(w_out))


def angle_tables():
    inverse = 10000.0 ** (-np.arange(HALF) * 2.0 / HEAD_DIM)
    angle = np.arange(BLOCK)[:, None] * inverse[None, :]
    return np.cos(angle).astype(np.float32), np.sin(angle).astype(np.float32)


def on_device(
    mix_query,
    mix_key,
    mix_value,
    mix_gate,
    log_decay,
    ret_gain,
    w_out,
    moe_in,
    route_ids,
    route_weights,
    moe_gain,
    w_gate,
    w_up,
    w_down,
):
    seq_rows = mix_query.shape[0]
    blocks = seq_rows // BLOCK
    width = moe_in.shape[1]
    ep = ("z", "x")
    tp = ("y", "core")

    ids = route_ids.T
    outgoing = pl.pallas_call(
        pre_kernel,
        out_shape=jax.ShapeDtypeStruct((SLOTS, width), bf16),
        compiler_params=pltpu.CompilerParams(vmem_limit_bytes=8 * MIB),
        cost_estimate=pl.CostEstimate(flops=2 * 10**9, bytes_accessed=10**6, transcendentals=0),
        name="pre",
    )(hb(moe_in), hb(ids), hb(moe_gain.reshape(1, -1)))
    own = lax.all_to_all(outgoing, ep, split_axis=0, concat_axis=0, tiled=True)

    cos_t, sin_t = angle_tables()
    inverse = 10000.0 ** (-np.arange(HALF) * 2.0 / HEAD_DIM)
    first = lax.axis_index(ep) * seq_rows + BLOCK * jnp.arange(blocks, dtype=jnp.int32)
    angle = first.astype(f32)[:, None] * jnp.asarray(inverse, f32)[None, :]
    base = jnp.stack([jnp.cos(angle), jnp.sin(angle)], axis=1)
    kept, qd, end = local_part(
        base,
        after(mix_query, outgoing),
        mix_key,
        mix_value,
        log_decay.reshape(blocks, 1, BLOCK),
        jnp.asarray(cos_t),
        jnp.asarray(sin_t),
    )
    by_x = [shift(end, "x", s) for s in (1, 2, 3)]
    own = after(own, end)

    up = shift(own, "y", 1)
    down = shift(own, "y", -1)
    far = shift(own, "y", 2)
    own_c = shift(own, "core", 1, 2)
    x_index = lax.axis_index("x").astype(jnp.int32).reshape(1)
    before, whole = middle(x_index, end, *by_x)
    by_z = [shift(whole, "z", s) for s in (1, 2, 3)]
    up_c = shift(up, "core", 1, 2)
    down_c = shift(down, "core", 1, 2)
    n = own.shape[0]
    weights = (w_gate[0], w_up[0], w_down[0])
    *keep, give1 = ffn([own, up, down], [own_c, up_c, down_c], weights)
    got1 = shift(give1, "core", 1, 2)
    far_c = shift(far, "core", 1, 2)
    near = sums([*keep, got1], tuple(((i, 0), (3, i * n)) for i in range(3)))
    back_up = shift(near[1], "y", -1)
    back_down = shift(near[2], "y", 1)
    keep2, give2 = ffn([after(far, near[2])], [far_c], weights)
    got2 = shift(give2, "core", 1, 2)
    (away,) = sums([keep2, got2], (((0, 0), (1, 0)),))
    back_far = shift(away, "y", 2)
    y_at, c_at = lax.axis_index("y"), lax.axis_index("core")
    place = jnp.stack([lax.axis_index("z"), y_at, c_at]).astype(jnp.int32)
    heads_out = finish(
        place, before, *by_z, kept, qd, mix_gate, ret_gain.reshape(1, -1)
    )
    pieces, sources = [], []
    m = seq_rows // 8
    for dy in range(4):
        for dc in range(2):
            at = (2 * dy + dc) * m
            piece = heads_out[at : at + m]
            if dy or dc:
                pairs = [
                    (2 * y + c, 2 * ((y + dy) % 4) + (c + dc) % 2)
                    for y in range(4)
                    for c in range(2)
                ]
                piece = lax.ppermute(piece, tp, pairs)
            pieces.append(piece)
            sources.append(2 * lax.rem(y_at - dy + 4, 4) + lax.rem(c_at + dc, 2))
    (expert_rows,) = sums(
        [near[0], back_up, back_down, back_far], (tuple((i, 0) for i in range(4)),)
    )
    returned = lax.all_to_all(expert_rows, ep, split_axis=0, concat_axis=0, tiled=True)
    mix_out = project(jnp.stack(sources).astype(jnp.int32), pieces, w_out)
    moe_out = pl.pallas_call(
        combine_kernel,
        out_shape=jax.ShapeDtypeStruct(moe_in.shape, bf16),
        compiler_params=pltpu.CompilerParams(vmem_limit_bytes=8 * MIB),
        cost_estimate=pl.CostEstimate(flops=10**9, bytes_accessed=10**6, transcendentals=0),
        name="combine",
    )(returned, ids, route_weights.T)
    return (mix_out, moe_out)


def solution(mesh):
    ep, tp = ("z", "x"), ("y", "core")
    every = ep + tp
    fine = Mesh(mesh.devices.reshape(4, 4, 4, 2), every)
    in_specs = (
        P(ep, tp),
        P(ep, tp),
        P(ep, tp),
        P(ep, tp),
        P(ep, tp),
        P(tp),
        P(),
        P(every, None),
        P(every, None),
        P(every, None),
        P(),
        P(ep, None, tp),
        P(ep, None, tp),
        P(ep, tp, None),
    )
    out_specs = (P(every, None), P(every, None))

    return jax.shard_map(
        on_device, mesh=fine, in_specs=in_specs, out_specs=out_specs, check_vma=False
    )
```
